512 devices in a mesh: ep: 32 (over z, x), tp: 16 (over y, core).
Axes of the slice: x: 4, y: 8, z: 8, core: 2. Of those that a mesh axis runs over, the one named last changes fastest.
Arguments:
- tokens: bfloat16 [768, 4096], P('ep'), may hold values from -6 to 6
- norm_gain: float32 [4096], replicated, may hold values from 0.1 to 1.9
- routes: int32 [768, 6], P('ep'), may hold values from 0 to 63, all different within a row; in each aligned block of 24 rows (0 to 23, 24 to 47, ...) at most 6 rows name the same one
- route_scores: float32 [768, 6], P('ep'), may hold values from 0.05 to 1
- expert_gate: bfloat16 [64, 1024, 4096], P('ep', 'tp'), may hold values from -0.09375 to 0.09375
- expert_up: bfloat16 [64, 1024, 4096], P('ep', 'tp'), may hold values from -0.09375 to 0.09375
- expert_down: bfloat16 [64, 1024, 4096], P('ep', 'tp'), may hold values from -0.1875 to 0.1875
- shared_gate: bfloat16 [1024, 4096], P('tp'), may hold values from -0.09375 to 0.09375
- shared_up: bfloat16 [1024, 4096], P('tp'), may hold values from -0.09375 to 0.09375
- shared_down: bfloat16 [1024, 4096], P('tp'), may hold values from -0.1875 to 0.1875
Outputs:
- mixed: bfloat16 [768, 4096], P('ep', 'tp')
The draws below stay inside these ranges and needn't reach their ends.
Inputs may be any that keep to these rules, and one draw needn't show every extreme that they name: `routes`: each row names 6 different experts. In the rows of one device (aligned blocks of 24 rows) no expert is named by more than 6 rows, and in some block one expert is named by exactly 6 rows.
All inputs are finite; a program needn't handle non-finite values.
Results may differ from the reference program's by a relative error of at most 0.02.
Values may be sent and summed in bfloat16 or wider, within the bound.
No kernel may reach another device: no remote copies, remote signals or barrier semaphores. Data moves between devices by JAX's collectives and lax.ppermute only.
A program may use at most 64 MiB of HBM per device.

```python
import math
import jax
import jax.numpy as jnp
import numpy as np
from jax import lax

D = 4096
FF = 1024
SFF = 1024
TOPK = 6
TOK_DEV = 24
EXPERTS = 64
CAP = 6
TOKENS = 768
N_EP = 32
N_TP = 16


def block_scale(stream_key, extent, cuts, low, high):
    def one(position, blocks):
        draws = jax.random.uniform(jax.random.fold_in(jax.random.fold_in(stream_key, 6), position), (blocks,), jnp.float32, low / len(cuts), high / len(cuts))
        return jnp.repeat(jnp.exp(draws), extent[position] // blocks).reshape((-1,) + (1,) * (len(extent) - position - 1))

    gain = one(*cuts[0])
    for cut in cuts[1:]:
        gain = gain * one(*cut)
    return gain


def shared_out(own_key, own, number, rows, amount, top, bound, skew):
    sequence = jax.random.permutation(own_key, amount)
    heavy_load, usual = shares(amount, rows * top, bound, skew, True), shares(amount, rows * top, bound, skew, False)
    places = jnp.arange(amount)

    def named(sizes, turn):
        used = int((sizes > 0).sum())
        fixed = max(1, used // 4)
        shifted = fixed + (places - fixed + turn * (used - fixed)) % max(1, amount - fixed)
        return jnp.zeros((amount,), jnp.int32).at[sequence[jnp.where(places < fixed, places, shifted)]].set(jnp.asarray(sizes, jnp.int32))

    sizes = jnp.where(number % 4 == 0, named(heavy_load, number // 4), named(usual, number - number // 4 - 1))
    mixed = jax.random.permutation(jax.random.fold_in(own, 3), amount)
    source_of, receiver = mixed[0:amount // 2 * 2:2], mixed[1:amount // 2 * 2:2]
    room = jnp.minimum(sizes[source_of] - 1, bound - sizes[receiver]) // 2
    room = jnp.where((source_of == sequence[0]) | (receiver == sequence[0]) | (sizes[receiver] == 0), 0, jnp.maximum(room, 0))
    shifted = jax.random.randint(jax.random.fold_in(own, 4), (amount // 2,), 0, 1 << 20) % (room + 1)
    sizes = sizes.at[source_of].add(-shifted).at[receiver].add(shifted)
    members = jnp.searchsorted(jnp.cumsum(sizes), jnp.arange(rows * top), side="right").astype(jnp.int32)
    listing = members.reshape(top, rows).T
    listing = listing[jax.random.permutation(jax.random.fold_in(own, 1), rows)]
    turn = jax.random.randint(jax.random.fold_in(own, 2), (rows, 1), 0, top)
    return jnp.take_along_axis(listing, (jnp.arange(top)[None, :] + turn) % top, axis=1)


def shares(number_of, total, bound, skew, full):
    weights = [(1 << 20) // math.isqrt(rank ** skew) + 1 for rank in range(1, number_of + 1)]
    largest = bound if full else min(bound, max(-(-total // number_of), total * weights[0] // sum(weights)))
    least = 1 if total - largest >= number_of - 1 else 0
    given, spare = [largest] + [least] * (number_of - 1), total - largest - least * (number_of - 1)
    while spare > 0:
        movable = [i for i in range(1, number_of) if given[i] < largest] or [i for i in range(1, number_of) if given[i] < bound]
        pool, left = sum([weights[i] for i in movable]), spare
        for i in movable:
            more = min(bound - given[i], max(1, left * weights[i] // pool), spare)
            given[i] = given[i] + more
            spare = spare - more
    return np.array(given)


def noise(stream_key, shape, scale, most, cuts=(), kind=jnp.bfloat16):
    array = scale * jax.random.normal(stream_key, shape, jnp.float32)
    if cuts:
        array = array * block_scale(stream_key, shape, cuts, -0.22, 0.18)
    return jnp.clip(array, -most, most).astype(kind)


def setup_inputs(seed: int = 0) -> dict:
    keys = jax.random.split(jax.random.key(seed), 11)
    tokens = noise(keys[0], (TOKENS, D), 1.0, 6.0, ((0, 32),))
    norm_gain = jnp.clip(1.0 + 0.18 * jax.random.normal(keys[1], (D,), jnp.float32), 0.1, 1.9)
    routes_keys = jax.random.split(jax.random.fold_in(keys[2], 1), TOKENS // TOK_DEV)
    routes_turns = jax.random.permutation(jax.random.fold_in(keys[2], 3), TOKENS // TOK_DEV)
    routes = jax.vmap(lambda own, number: shared_out(jax.random.fold_in(keys[2], 2), own, number, TOK_DEV, EXPERTS, TOPK, CAP, 2))(routes_keys, routes_turns).reshape((TOKENS, TOPK))
    route_scores = jnp.clip(0.05 + 0.95 * jax.random.uniform(keys[3], (TOKENS, TOPK), jnp.float32) ** block_scale(keys[3], (TOKENS, TOPK), ((0, 32),), -0.2, 0.2), 0.05, 1.0)
    expert_gate = noise(keys[4], (EXPERTS, FF, D), D ** -0.5, 0.09375, ((0, 32), (1, 16)))
    expert_up = noise(keys[5], (EXPERTS, FF, D), D ** -0.5, 0.09375, ((0, 32), (1, 16)))
    expert_down = noise(keys[6], (EXPERTS, FF, D), FF ** -0.5, 0.1875, ((0, 32), (1, 16)))
    shared_gate = noise(keys[7], (SFF, D), D ** -0.5, 0.09375, ((0, 16),))
    shared_up = noise(keys[8], (SFF, D), D ** -0.5, 0.09375, ((0, 16),))
    shared_down = noise(keys[9], (SFF, D), SFF ** -0.5, 0.1875, ((0, 16),))
    return dict(tokens=tokens, norm_gain=norm_gain, routes=routes, route_scores=route_scores, expert_gate=expert_gate, expert_up=expert_up, expert_down=expert_down, shared_gate=shared_gate, shared_up=shared_up, shared_down=shared_down)


def slot_index(route_block):
    flat = route_block.reshape(-1)
    onehot = (flat[:, None] == jnp.arange(EXPERTS, dtype=jnp.int32)[None, :]).astype(jnp.int32)
    before = jnp.cumsum(onehot, 0) - onehot
    order = lax.optimization_barrier(jnp.sum(before * onehot, 1))
    return (flat * CAP + order).astype(jnp.int32).reshape(route_block.shape)

def group_sum(hidden, down):
    rows = hidden.shape[0]
    width = down.shape[1]
    left = hidden.astype(jnp.float32).reshape(rows, N_TP, -1)
    right = down.astype(jnp.float32).reshape(N_TP, -1, width)
    parts = jnp.einsum('rnf,nfd->nrd', left, right)
    return lax.optimization_barrier(jnp.sum(parts.astype(jnp.bfloat16).astype(jnp.float32), 0))

def swiglu_sum(rows, gate_w, up_w, down_w):
    gate = jnp.dot(rows, gate_w.T, preferred_element_type=jnp.float32)
    upper = jnp.dot(rows, up_w.T, preferred_element_type=jnp.float32)
    hidden = (jax.nn.silu(gate) * upper).astype(jnp.bfloat16)
    return group_sum(hidden, down_w)

def reference(tokens, norm_gain, routes, route_scores, expert_gate, expert_up, expert_down, shared_gate, shared_up, shared_down):
    values = tokens.astype(jnp.float32)
    normed = (values * lax.rsqrt(lax.optimization_barrier(jnp.mean(values * values, -1, keepdims=True)) + 1e-06) * norm_gain).astype(jnp.bfloat16)
    blocks = routes.reshape(N_EP, TOK_DEV, TOPK)
    slots = jax.vmap(slot_index)(blocks)
    source = jnp.broadcast_to(jnp.arange(N_EP, dtype=jnp.int32)[:, None, None], slots.shape)
    rows = jnp.broadcast_to(normed.reshape(N_EP, TOK_DEV, 1, D), (N_EP, TOK_DEV, TOPK, D))
    buffer = jnp.zeros((N_EP, EXPERTS * CAP, D), jnp.bfloat16).at[source, slots].set(rows)
    per_expert = buffer.reshape(N_EP, EXPERTS, CAP, D).transpose(1, 0, 2, 3).reshape(EXPERTS, N_EP * CAP, D)

    def one_expert(items):
        return swiglu_sum(items[0], items[1], items[2], items[3]).astype(jnp.bfloat16)
    outs = lax.map(one_expert, (per_expert, expert_gate, expert_up, expert_down))
    outs = outs.reshape(EXPERTS, N_EP, CAP, D).transpose(1, 0, 2, 3).reshape(N_EP, EXPERTS * CAP, D)
    picked = outs[source, slots].astype(jnp.float32)
    weights = route_scores / lax.optimization_barrier(jnp.sum(route_scores, -1, keepdims=True)) * 2.5
    routed = lax.optimization_barrier(jnp.sum(weights.reshape(N_EP, TOK_DEV, TOPK, 1) * picked, 2)).reshape(TOKENS, D)
    shared = swiglu_sum(normed, shared_gate, shared_up, shared_down)
    return (shared + routed).astype(jnp.bfloat16)
```

```python
import jax
import jax.numpy as jnp
from jax import lax
from jax.experimental import pallas as pl
from jax.experimental.pallas import tpu as pltpu
from jax.sharding import Mesh, PartitionSpec as P


NZ, NX, NY, NC = 8, 4, 8, 2
EP = NZ * NX
D = 4096
FF_DEV = 64
TOK = 24
TOPK = 6
EXPERTS = 64
CAP = 6
QUARTERS = 4
QW = D // QUARTERS
PIECE = CAP * QUARTERS
ROWS = EP * PIECE
SLOTS = EP * CAP
OUT_W = D // NY
HALF = OUT_W // NC
LANES = 128
GROUP = 32
NGROUPS = SLOTS // GROUP
MSG = NC * FF_DEV + TOK
VM = pl.BlockSpec(memory_space=pltpu.VMEM)
F32, BF16 = jnp.float32, jnp.bfloat16


def iota(shape, dim):
    return lax.broadcasted_iota(jnp.int32, shape, dim)


def nt(a, b):
    return lax.dot_general(a, b, (((1,), (1,)), ((), ())), preferred_element_type=F32)


def nn(a, b):
    return jnp.dot(a, b, preferred_element_type=F32)


def membership(routes):
    named = jnp.zeros((TOK, EXPERTS), F32)
    for k in range(TOPK):
        named += (routes[:, k : k + 1] == iota((TOK, EXPERTS), 1)).astype(F32)
    earlier = (iota((TOK, TOK), 1) < iota((TOK, TOK), 0)).astype(F32)
    rank = nn(earlier.astype(BF16), named.astype(BF16))
    code = named * (rank + 1.0 + (CAP * (iota((TOK, EXPERTS), 1) >> 1)).astype(F32))
    return code


def pack_kernel(tok_ref, gain_ref, routes_ref, send_ref, normed_ref, stack_ref, code_ref):
    core = lax.axis_index("c")
    values = tok_ref[...].astype(F32)
    normed = (
        values * lax.rsqrt(jnp.mean(values * values, -1, keepdims=True) + 1e-06) * gain_ref[...]
    ).astype(BF16)
    normed_ref[...] = normed
    code = membership(routes_ref[...])
    stack_ref[...] = jnp.zeros(stack_ref.shape, BF16)
    code_ref[...] = jnp.zeros(code_ref.shape, F32)
    for q in range(QUARTERS):
        stack_ref[q * GROUP : q * GROUP + TOK, :] = normed[:, q * QW : (q + 1) * QW]
        code_ref[q * GROUP : q * GROUP + TOK, :] = code
    row, expert = iota((ROWS, EXPERTS), 0), iota((ROWS, EXPERTS), 1)
    low = (expert - core) * (PIECE // 2)
    owner = ((expert & 1) == core) & (row >= low) & (row < low + PIECE)
    found = nt(owner.astype(F32).astype(BF16), code_ref[...].astype(BF16))
    row, col = iota((ROWS, LANES), 0), iota((ROWS, LANES), 1)
    table = (found == ((row >> 2) + 1).astype(F32)) & ((row & 3) == (col >> 5))
    table = table.astype(F32).astype(BF16)
    chunk = ROWS // 4
    for k in range(4):
        send_ref[k * chunk : (k + 1) * chunk, :] = nn(
            table[k * chunk : (k + 1) * chunk, :], stack_ref[...]
        ).astype(BF16)


def side_kernel(
    normed_ref, routes_ref, scores_ref, sg_ref, su_ref, sd_ref, own_ref, got_ref, *refs
):
    messages, (chi_ref, clo_ref, part_ref, code_ref, weight_ref) = refs[:NY], refs[NY:]
    core, me = lax.axis_index("c"), lax.axis_index("y")
    normed = normed_ref[...]
    gate, upper = nt(normed, sg_ref[...]), nt(normed, su_ref[...])
    hidden = (gate / (1.0 + jnp.exp(-gate)) * upper).astype(BF16)
    part_ref[...] = nn(hidden, sd_ref[...]).astype(BF16)
    for d in range(NY):
        cols = pl.ds(pl.multiple_of(lax.rem(me + d, NY) * OUT_W, OUT_W), OUT_W)
        messages[d][0:FF_DEV, :] = own_ref[2 * FF_DEV : 3 * FF_DEV, cols]
        messages[d][FF_DEV : 2 * FF_DEV, :] = got_ref[2 * FF_DEV : 3 * FF_DEV, cols]
        messages[d][2 * FF_DEV : MSG, :] = part_ref[:, cols]
    routes, scores = routes_ref[...], scores_ref[...]
    code = membership(routes)
    weights = scores / jnp.sum(scores, -1, keepdims=True) * 2.5
    spread = jnp.zeros((TOK, EXPERTS), F32)
    for k in range(TOPK):
        spread += jnp.where(
            routes[:, k : k + 1] == iota((TOK, EXPERTS), 1), weights[:, k : k + 1], 0.0
        )
    code_ref[...] = jnp.zeros(code_ref.shape, F32)
    weight_ref[...] = jnp.zeros(weight_ref.shape, F32)
    for q in range(QUARTERS):
        code_ref[q * GROUP : q * GROUP + TOK, :] = code
        weight_ref[q * GROUP : q * GROUP + TOK, :] = spread
    expert, row = iota((EXPERTS, ROWS), 0), iota((EXPERTS, ROWS), 1)
    low = (expert - core) * (PIECE // 2)
    owner = ((expert & 1) == core) & (row >= low) & (row < low + PIECE)
    owner = owner.astype(F32).astype(BF16)
    found = nn(code_ref[...].astype(BF16), owner)
    token, row = iota((LANES, ROWS), 0), iota((LANES, ROWS), 1)
    table = (found == ((row >> 2) + 1).astype(F32)) & ((row & 3) == (token >> 5))
    weight = weight_ref[...]
    high = weight.astype(BF16)
    rest = (weight - high.astype(F32)).astype(BF16)
    chi_ref[...] = jnp.where(table, nn(high, owner), 0.0).astype(BF16)
    clo_ref[...] = jnp.where(table, nn(rest, owner), 0.0).astype(BF16)


def hidden_kernel(rows_ref, own_ref, got_ref, out_ref, x_ref):
    i, j = iota((LANES, LANES), 0), iota((LANES, LANES), 1)
    sort = (j == (i & (GROUP - 1)) * QUARTERS + (i >> 5)).astype(F32).astype(BF16)
    for g in range(NGROUPS):
        block = nn(sort, rows_ref[g * LANES : (g + 1) * LANES, :]).astype(BF16)
        for q in range(QUARTERS):
            x_ref[g * GROUP : (g + 1) * GROUP, q * QW : (q + 1) * QW] = block[
                q * GROUP : (q + 1) * GROUP, :
            ]
    parts = []
    for ref in (own_ref, got_ref):
        both = nt(x_ref[...], ref[0 : 2 * FF_DEV, :])
        gate, upper = both[:, :FF_DEV], both[:, FF_DEV:]
        parts.append(gate / (1.0 + jnp.exp(-gate)) * upper)
    hidden = jnp.concatenate(parts, axis=1).astype(BF16)
    for d in range(NY):
        out_ref[d] = hidden


def down_kernel(hidden_ref, *refs):
    messages, (out_ref, shared_ref, stack_ref) = refs[:NY], refs[NY:]
    me = lax.axis_index("y")
    total = jnp.zeros((SLOTS, OUT_W), F32)
    shared = jnp.zeros((TOK, OUT_W), F32)
    for d in range(NY):
        source = lax.rem(me + NY - d, NY)
        total += nn(hidden_ref[source], messages[d][0 : 2 * FF_DEV, :])
        shared += messages[d][2 * FF_DEV : MSG, :].astype(F32)
    shared_ref[...] = shared
    done = total.astype(BF16)
    for g in range(NGROUPS):
        for q in range(QUARTERS):
            stack_ref[g * LANES + q * GROUP : g * LANES + (q + 1) * GROUP, :] = done[
                g * GROUP : (g + 1) * GROUP, q * LANES : (q + 1) * LANES
            ]
    i, j = iota((LANES, LANES), 0), iota((LANES, LANES), 1)
    sort = (j == (i & 3) * GROUP + (i >> 2)).astype(F32).astype(BF16)
    for g in range(NGROUPS):
        rows = slice(g * LANES, (g + 1) * LANES)
        out_ref[rows, :] = nn(sort, stack_ref[rows, :]).astype(BF16)


def combine_kernel(rows_ref, chi_ref, clo_ref, shared_ref, mine_ref, other_ref, acc_ref):
    core = lax.axis_index("c")
    acc_ref[...] = nn(chi_ref[...], rows_ref[...]) + nn(clo_ref[...], rows_ref[...])
    per = HALF // LANES
    for half in range(NC):
        whole = jnp.concatenate(
            [
                acc_ref[q * GROUP : q * GROUP + TOK, :]
                + shared_ref[:, q * LANES : (q + 1) * LANES]
                for q in range(half * per, (half + 1) * per)
            ],
            axis=1,
        )

        @pl.when(core == half)
        def _():
            mine_ref[...] = whole

        @pl.when(core != half)
        def _():
            other_ref[...] = whole


def call(kernel, outs, scratch, flops, *args):
    return pl.pallas_call(
        kernel,
        out_shape=outs,
        in_specs=[VM] * len(args),
        out_specs=jax.tree.map(lambda _: VM, outs),
        scratch_shapes=scratch,
        compiler_params=pltpu.CompilerParams(vmem_limit_bytes=24 << 20),
        cost_estimate=pl.CostEstimate(flops=flops, bytes_accessed=1 << 20, transcendentals=0),
    )(*args)


def out(shape, dtype=BF16):
    return jax.ShapeDtypeStruct(shape, dtype)


def hop(x, axis, size, step):
    return lax.ppermute(x, axis, [(i, (i + step) % size) for i in range(size)])


def body(
    tokens,
    norm_gain,
    routes,
    route_scores,
    expert_gate,
    expert_up,
    expert_down,
    shared_gate,
    shared_up,
    shared_down,
):
    core = lax.axis_index("c")

    def of(which):
        return jnp.concatenate(
            [
                lax.dynamic_index_in_dim(w, which, 0, keepdims=False)
                for w in (expert_gate, expert_up, expert_down)
            ],
            axis=0,
        )

    got = hop(of(1 - core), "c", NC, 1)
    own = of(core)
    send, normed = call(
        pack_kernel,
        (out((ROWS, QW)), out((TOK, D))),
        [pltpu.VMEM((LANES, QW), BF16), pltpu.VMEM((LANES, EXPERTS), F32)],
        1 << 30,
        tokens,
        norm_gain.reshape(1, D),
        routes,
    )
    rows = lax.all_to_all(
        send.reshape(EP, PIECE, QW), ("z", "x"), split_axis=0, concat_axis=0, tiled=True
    ).reshape(ROWS, QW)
    *messages, chi, clo = call(
        side_kernel,
        tuple(out((MSG, OUT_W)) for _ in range(NY)) + (out((LANES, ROWS)), out((LANES, ROWS))),
        [
            pltpu.VMEM((TOK, D), BF16),
            pltpu.VMEM((LANES, EXPERTS), F32),
            pltpu.VMEM((LANES, EXPERTS), F32),
        ],
        1 << 30,
        normed,
        routes,
        route_scores,
        shared_gate,
        shared_up,
        shared_down,
        own,
        got,
    )
    messages = [messages[0]] + [hop(messages[d], "y", NY, d) for d in range(1, NY)]
    hidden = call(
        hidden_kernel,
        out((NY, SLOTS, 2 * FF_DEV)),
        [pltpu.VMEM((SLOTS, D), BF16)],
        1 << 30,
        rows,
        own,
        got,
    )
    hidden = lax.all_to_all(hidden, "y", split_axis=0, concat_axis=0, tiled=True)
    back, shared = call(
        down_kernel,
        (out((ROWS, LANES)), out((TOK, OUT_W), F32)),
        [pltpu.VMEM((ROWS, LANES), BF16)],
        1 << 30,
        hidden,
        *messages,
    )
    back = lax.all_to_all(
        back.reshape(EP, PIECE, LANES), ("z", "x"), split_axis=0, concat_axis=0, tiled=True
    ).reshape(ROWS, LANES)
    mine, other = call(
        combine_kernel,
        (out((TOK, HALF), F32), out((TOK, HALF), F32)),
        [pltpu.VMEM((LANES, LANES), F32)],
        1 << 28,
        back,
        chi,
        clo,
        shared,
    )
    return (mine + hop(other, "c", NC, 1)).astype(BF16)


def solution(mesh):
    fine = Mesh(mesh.devices.reshape(NZ, NX, NY, NC), ("z", "x", "y", "c"))
    ep, tp = ("z", "x"), ("y", "c")
    in_specs = (
        P(ep, None),
        P(),
        P(ep, None),
        P(ep, None),
        P(ep, tp, None),
        P(ep, tp, None),
        P(ep, tp, None),
        P(tp, None),
        P(tp, None),
        P(tp, None),
    )
    return jax.shard_map(
        body, mesh=fine, in_specs=in_specs, out_specs=P(ep, tp), check_vma=False
    )
```

```python
import jax
import jax.numpy as jnp
from jax import lax
from jax.experimental import pallas as pl
from jax.experimental.pallas import tpu as pltpu
from jax.sharding import Mesh, PartitionSpec as P


NZ, NX, NY, NC = 8, 4, 8, 2
EP = NZ * NX
D = 4096
FF_DEV = 64
TOK = 24
TOPK = 6
EXPERTS = 64
CAP = 6
QUARTERS = 4
QW = D // QUARTERS
PIECE = CAP * QUARTERS
ROWS = EP * PIECE
SLOTS = EP * CAP
OUT_W = D // NY
HALF = OUT_W // NC
LANES = 128
GROUP = 32
NGROUPS = SLOTS // GROUP
MSG = NC * FF_DEV + TOK
VM = pl.BlockSpec(memory_space=pltpu.VMEM)
F32, BF16 = jnp.float32, jnp.bfloat16


def iota(shape, dim):
    return lax.broadcasted_iota(jnp.int32, shape, dim)


def nt(a, b):
    return lax.dot_general(a, b, (((1,), (1,)), ((), ())), preferred_element_type=F32)


def nn(a, b):
    return jnp.dot(a, b, preferred_element_type=F32)


def membership(routes):
    named = jnp.zeros((TOK, EXPERTS), F32)
    for k in range(TOPK):
        named += (routes[:, k : k + 1] == iota((TOK, EXPERTS), 1)).astype(F32)
    earlier = (iota((TOK, TOK), 1) < iota((TOK, TOK), 0)).astype(F32)
    rank = nn(earlier.astype(BF16), named.astype(BF16))
    code = named * (rank + 1.0 + (CAP * (iota((TOK, EXPERTS), 1) >> 1)).astype(F32))
    return code


def pack_kernel(tok_ref, gain_ref, routes_ref, send_ref, normed_ref, stack_ref, code_ref):
    core = lax.axis_index("c")
    values = tok_ref[...].astype(F32)
    normed = (
        values * lax.rsqrt(jnp.mean(values * values, -1, keepdims=True) + 1e-06) * gain_ref[...]
    ).astype(BF16)
    normed_ref[...] = normed
    code = membership(routes_ref[...])
    stack_ref[...] = jnp.zeros(stack_ref.shape, BF16)
    code_ref[...] = jnp.zeros(code_ref.shape, F32)
    for q in range(QUARTERS):
        stack_ref[q * GROUP : q * GROUP + TOK, :] = normed[:, q * QW : (q + 1) * QW]
        code_ref[q * GROUP : q * GROUP + TOK, :] = code
    row, expert = iota((ROWS, EXPERTS), 0), iota((ROWS, EXPERTS), 1)
    low = (expert - core) * (PIECE // 2)
    owner = ((expert & 1) == core) & (row >= low) & (row < low + PIECE)
    found = nt(owner.astype(F32).astype(BF16), code_ref[...].astype(BF16))
    row, col = iota((ROWS, LANES), 0), iota((ROWS, LANES), 1)
    table = (found == ((row >> 2) + 1).astype(F32)) & ((row & 3) == (col >> 5))
    table = table.astype(F32).astype(BF16)
    chunk = ROWS // 4
    for k in range(4):
        send_ref[k * chunk : (k + 1) * chunk, :] = nn(
            table[k * chunk : (k + 1) * chunk, :], stack_ref[...]
        ).astype(BF16)


def side_kernel(
    normed_ref, routes_ref, scores_ref, sg_ref, su_ref, sd_ref, own_ref, got_ref, *refs
):
    messages, (chi_ref, clo_ref, part_ref, code_ref, weight_ref) = refs[:NY], refs[NY:]
    core, me = lax.axis_index("c"), lax.axis_index("y")
    normed = normed_ref[...]
    gate, upper = nt(normed, sg_ref[...]), nt(normed, su_ref[...])
    hidden = (gate / (1.0 + jnp.exp(-gate)) * upper).astype(BF16)
    part_ref[...] = nn(hidden, sd_ref[...]).astype(BF16)
    for d in range(NY):
        cols = pl.ds(pl.multiple_of(lax.rem(me + d, NY) * OUT_W, OUT_W), OUT_W)
        messages[d][0:FF_DEV, :] = own_ref[2 * FF_DEV : 3 * FF_DEV, cols]
        messages[d][FF_DEV : 2 * FF_DEV, :] = got_ref[2 * FF_DEV : 3 * FF_DEV, cols]
        messages[d][2 * FF_DEV : MSG, :] = part_ref[:, cols]
    routes, scores = routes_ref[...], scores_ref[...]
    code = membership(routes)
    weights = scores / jnp.sum(scores, -1, keepdims=True) * 2.5
    spread = jnp.zeros((TOK, EXPERTS), F32)
    for k in range(TOPK):
        spread += jnp.where(
            routes[:, k : k + 1] == iota((TOK, EXPERTS), 1), weights[:, k : k + 1], 0.0
        )
    code_ref[...] = jnp.zeros(code_ref.shape, F32)
    weight_ref[...] = jnp.zeros(weight_ref.shape, F32)
    for q in range(QUARTERS):
        code_ref[q * GROUP : q * GROUP + TOK, :] = code
        weight_ref[q * GROUP : q * GROUP + TOK, :] = spread
    expert, row = iota((EXPERTS, ROWS), 0), iota((EXPERTS, ROWS), 1)
    low = (expert - core) * (PIECE // 2)
    owner = ((expert & 1) == core) & (row >= low) & (row < low + PIECE)
    owner = owner.astype(F32).astype(BF16)
    found = nn(code_ref[...].astype(BF16), owner)
    token, row = iota((LANES, ROWS), 0), iota((LANES, ROWS), 1)
    table = (found == ((row >> 2) + 1).astype(F32)) & ((row & 3) == (token >> 5))
    weight = weight_ref[...]
    high = weight.astype(BF16)
    rest = (weight - high.astype(F32)).astype(BF16)
    chi_ref[...] = jnp.where(table, nn(high, owner), 0.0).astype(BF16)
    clo_ref[...] = jnp.where(table, nn(rest, owner), 0.0).astype(BF16)


def hidden_kernel(rows_ref, own_ref, got_ref, out_ref, x_ref):
    i, j = iota((LANES, LANES), 0), iota((LANES, LANES), 1)
    sort = (j == (i & (GROUP - 1)) * QUARTERS + (i >> 5)).astype(F32).astype(BF16)
    for g in range(NGROUPS):
        block = nn(sort, rows_ref[g * LANES : (g + 1) * LANES, :]).astype(BF16)
        for q in range(QUARTERS):
            x_ref[g * GROUP : (g + 1) * GROUP, q * QW : (q + 1) * QW] = block[
                q * GROUP : (q + 1) * GROUP, :
            ]
    parts = []
    for ref in (own_ref, got_ref):
        both = nt(x_ref[...], ref[0 : 2 * FF_DEV, :])
        gate, upper = both[:, :FF_DEV], both[:, FF_DEV:]
        parts.append(gate / (1.0 + jnp.exp(-gate)) * upper)
    hidden = jnp.concatenate(parts, axis=1).astype(BF16)
    for d in range(NY):
        out_ref[d] = hidden


def down_kernel(hidden_ref, *refs):
    messages, (out_ref, shared_ref, stack_ref) = refs[:NY], refs[NY:]
    me = lax.axis_index("y")
    total = jnp.zeros((SLOTS, OUT_W), F32)
    shared = jnp.zeros((TOK, OUT_W), F32)
    for d in range(NY):
        source = lax.rem(me + NY - d, NY)
        total += nn(hidden_ref[source], messages[d][0 : 2 * FF_DEV, :])
        shared += messages[d][2 * FF_DEV : MSG, :].astype(F32)
    shared_ref[...] = shared
    done = total.astype(BF16)
    for g in range(NGROUPS):
        for q in range(QUARTERS):
            stack_ref[g * LANES + q * GROUP : g * LANES + (q + 1) * GROUP, :] = done[
                g * GROUP : (g + 1) * GROUP, q * LANES : (q + 1) * LANES
            ]
    i, j = iota((LANES, LANES), 0), iota((LANES, LANES), 1)
    sort = (j == (i & 3) * GROUP + (i >> 2)).astype(F32).astype(BF16)
    for g in range(NGROUPS):
        rows = slice(g * LANES, (g + 1) * LANES)
        out_ref[rows, :] = nn(sort, stack_ref[rows, :]).astype(BF16)


def combine_kernel(rows_ref, chi_ref, clo_ref, shared_ref, mine_ref, other_ref, acc_ref):
    core = lax.axis_index("c")
    acc_ref[...] = nn(chi_ref[...], rows_ref[...]) + nn(clo_ref[...], rows_ref[...])
    per = HALF // LANES
    for half in range(NC):
        whole = jnp.concatenate(
            [
                acc_ref[q * GROUP : q * GROUP + TOK, :]
                + shared_ref[:, q * LANES : (q + 1) * LANES]
                for q in range(half * per, (half + 1) * per)
            ],
            axis=1,
        )

        @pl.when(core == half)
        def _():
            mine_ref[...] = whole

        @pl.when(core != half)
        def _():
            other_ref[...] = whole


def call(kernel, outs, scratch, flops, *args):
    return pl.pallas_call(
        kernel,
        out_shape=outs,
        in_specs=[VM] * len(args),
        out_specs=jax.tree.map(lambda _: VM, outs),
        scratch_shapes=scratch,
        compiler_params=pltpu.CompilerParams(vmem_limit_bytes=24 << 20),
        cost_estimate=pl.CostEstimate(flops=flops, bytes_accessed=1 << 20, transcendentals=0),
    )(*args)


def out(shape, dtype=BF16):
    return jax.ShapeDtypeStruct(shape, dtype)


def hop(x, axis, size, step):
    return lax.ppermute(x, axis, [(i, (i + step) % size) for i in range(size)])


def body(
    tokens,
    norm_gain,
    routes,
    route_scores,
    expert_gate,
    expert_up,
    expert_down,
    shared_gate,
    shared_up,
    shared_down,
):
    core = lax.axis_index("c")

    def of(which):
        return jnp.concatenate(
            [
                lax.dynamic_index_in_dim(w, which, 0, keepdims=False)
                for w in (expert_gate, expert_up, expert_down)
            ],
            axis=0,
        )

    got = hop(of(1 - core), "c", NC, 1)
    own = of(core)
    send, normed = call(
        pack_kernel,
        (out((ROWS, QW)), out((TOK, D))),
        [pltpu.VMEM((LANES, QW), BF16), pltpu.VMEM((LANES, EXPERTS), F32)],
        1 << 30,
        tokens,
        norm_gain.reshape(1, D),
        routes,
    )
    rows = lax.all_to_all(
        send.reshape(EP, PIECE, QW), ("z", "x"), split_axis=0, concat_axis=0, tiled=True
    ).reshape(ROWS, QW)
    *messages, chi, clo = call(
        side_kernel,
        tuple(out((MSG, OUT_W)) for _ in range(NY)) + (out((LANES, ROWS)), out((LANES, ROWS))),
        [
            pltpu.VMEM((TOK, D), BF16),
            pltpu.VMEM((LANES, EXPERTS), F32),
            pltpu.VMEM((LANES, EXPERTS), F32),
        ],
        1 << 30,
        normed,
        routes,
        route_scores,
        shared_gate,
        shared_up,
        shared_down,
        own,
        got,
    )
    messages = [messages[0]] + [hop(messages[d], "y", NY, d) for d in range(1, NY)]
    rows, messages = lax.optimization_barrier((rows, messages))
    hidden = call(
        hidden_kernel,
        out((NY, SLOTS, 2 * FF_DEV)),
        [pltpu.VMEM((SLOTS, D), BF16)],
        1 << 30,
        rows,
        own,
        got,
    )
    hidden = lax.all_to_all(hidden, "y", split_axis=0, concat_axis=0, tiled=True)
    back, shared = call(
        down_kernel,
        (out((ROWS, LANES)), out((TOK, OUT_W), F32)),
        [pltpu.VMEM((ROWS, LANES), BF16)],
        1 << 30,
        hidden,
        *messages,
    )
    back = lax.all_to_all(
        back.reshape(EP, PIECE, LANES), ("z", "x"), split_axis=0, concat_axis=0, tiled=True
    ).reshape(ROWS, LANES)
    mine, other = call(
        combine_kernel,
        (out((TOK, HALF), F32), out((TOK, HALF), F32)),
        [pltpu.VMEM((LANES, LANES), F32)],
        1 << 28,
        back,
        chi,
        clo,
        shared,
    )
    return (mine + hop(other, "c", NC, 1)).astype(BF16)


def solution(mesh):
    fine = Mesh(mesh.devices.reshape(NZ, NX, NY, NC), ("z", "x", "y", "c"))
    ep, tp = ("z", "x"), ("y", "c")
    in_specs = (
        P(ep, None),
        P(),
        P(ep, None),
        P(ep, None),
        P(ep, tp, None),
        P(ep, tp, None),
        P(ep, tp, None),
        P(tp, None),
        P(tp, None),
        P(tp, None),
    )
    return jax.shard_map(
        body, mesh=fine, in_specs=in_specs, out_specs=P(ep, tp), check_vma=False
    )
```

```python
import jax
import jax.numpy as jnp
from jax import lax
from jax.experimental import pallas as pl
from jax.experimental.pallas import tpu as pltpu
from jax.sharding import Mesh, PartitionSpec as P


NZ, NX, NY, NC = 8, 4, 8, 2
EP = NZ * NX
D = 4096
FF_DEV = 64
TOK = 24
TOPK = 6
EXPERTS = 64
CAP = 6
QUARTERS = 4
QW = D // QUARTERS
PIECE = CAP * QUARTERS
ROWS = EP * PIECE
SLOTS = EP * CAP
OUT_W = D // NY
HALF = OUT_W // NC
LANES = 128
GROUP = 32
NGROUPS = SLOTS // GROUP
MSG = NC * FF_DEV + TOK
ORDER = (0, 4, 5, 3, 6, 2, 7, 1)
VM = pl.BlockSpec(memory_space=pltpu.VMEM)
HB = pl.BlockSpec(memory_space=pltpu.HBM)
F32, BF16 = jnp.float32, jnp.bfloat16


def iota(shape, dim):
    return lax.broadcasted_iota(jnp.int32, shape, dim)


def nt(a, b):
    return lax.dot_general(a, b, (((1,), (1,)), ((), ())), preferred_element_type=F32)


def nn(a, b):
    return jnp.dot(a, b, preferred_element_type=F32)


def spread_tokens(values):
    lane, token = iota((TOK, LANES), 1), iota((TOK, LANES), 0)
    place = ((lane & (GROUP - 1)) == token).astype(F32).astype(BF16)
    return nn(values.astype(BF16), place)


def membership(routes):
    named = jnp.zeros((EXPERTS, TOK), F32)
    for k in range(TOPK):
        named += (routes[k : k + 1, :] == iota((EXPERTS, TOK), 0)).astype(F32)
    earlier = (iota((TOK, TOK), 0) < iota((TOK, TOK), 1)).astype(F32)
    rank = nn(named.astype(BF16), earlier.astype(BF16))
    return named * (rank + 1.0 + (CAP * (iota((EXPERTS, TOK), 0) >> 1)).astype(F32))


def pack_kernel(
    tok_hbm, gain_hbm, routes_hbm, send_ref, normed_ref, stack_ref, tok_ref, gain_ref, routes_ref, sems
):
    core = lax.axis_index("c")
    routes_copy = pltpu.make_async_copy(routes_hbm, routes_ref, sems.at[2])
    tok_copy = pltpu.make_async_copy(tok_hbm, tok_ref, sems.at[0])
    gain_copy = pltpu.make_async_copy(gain_hbm, gain_ref, sems.at[1])
    routes_copy.start()
    tok_copy.start()
    gain_copy.start()
    routes_copy.wait()
    code = spread_tokens(membership(routes_ref[...])).astype(BF16)
    row, expert = iota((ROWS, EXPERTS), 0), iota((ROWS, EXPERTS), 1)
    low = (expert - core) * (PIECE // 2)
    owner = ((expert & 1) == core) & (row >= low) & (row < low + PIECE)
    found = nn(owner.astype(F32).astype(BF16), code)
    row, col = iota((ROWS, LANES), 0), iota((ROWS, LANES), 1)
    table = (found == ((row >> 2) + 1).astype(F32)) & ((row & 3) == (col >> 5))
    table = table.astype(F32).astype(BF16)
    stack_ref[...] = jnp.zeros(stack_ref.shape, BF16)
    tok_copy.wait()
    gain_copy.wait()
    values = tok_ref[...].astype(F32)
    normed = (
        values * lax.rsqrt(jnp.mean(values * values, -1, keepdims=True) + 1e-06) * gain_ref[...]
    ).astype(BF16)
    normed_ref[...] = normed
    for q in range(QUARTERS):
        stack_ref[q * GROUP : q * GROUP + TOK, :] = normed[:, q * QW : (q + 1) * QW]
    chunk = ROWS // 4
    for k in range(4):
        send_ref[k * chunk : (k + 1) * chunk, :] = nn(
            table[k * chunk : (k + 1) * chunk, :], stack_ref[...]
        ).astype(BF16)


def side_kernel(normed_ref, sg_ref, su_ref, sd_ref, down_ref, *refs):
    messages, part_ref = refs[:NY], refs[NY]
    me = lax.axis_index("y")
    normed = normed_ref[...]
    gate, upper = nt(normed, sg_ref[...]), nt(normed, su_ref[...])
    hidden = (gate / (1.0 + jnp.exp(-gate)) * upper).astype(BF16)
    part_ref[...] = nn(hidden, sd_ref[...]).astype(BF16)
    for d in range(NY):
        cols = pl.ds(pl.multiple_of(lax.rem(me + d, NY) * OUT_W, OUT_W), OUT_W)
        messages[d][0:FF_DEV, :] = down_ref[0, :, cols]
        messages[d][FF_DEV : 2 * FF_DEV, :] = down_ref[1, :, cols]
        messages[d][2 * FF_DEV : MSG, :] = part_ref[:, cols]


def ready_kernel(*refs):
    messages, (keep_ref, give_ref, shared_ref) = dict(zip(ORDER, refs)), refs[NY:]
    core, me = lax.axis_index("c"), lax.axis_index("y")
    shared = jnp.zeros((TOK, OUT_W), F32)
    for d in range(NY):
        source = lax.rem(me + NY - d, NY)
        rows = pl.ds(pl.multiple_of(source * FF_DEV, FF_DEV), FF_DEV)
        keep_ref[rows, :] = messages[d][pl.ds(pl.multiple_of(core * FF_DEV, FF_DEV), FF_DEV), :]
        give_ref[rows, :] = messages[d][
            pl.ds(pl.multiple_of((1 - core) * FF_DEV, FF_DEV), FF_DEV), :
        ]
        shared += messages[d][2 * FF_DEV : MSG, :].astype(F32)
    shared_ref[...] = shared


def hidden_kernel(
    rows_ref, gate_hbm, got_gate_hbm, up_hbm, got_up_hbm, after_hbm, out_ref, x_ref, weight_ref, sems
):
    core = lax.axis_index("c")
    copies = [
        pltpu.make_async_copy(
            ref.at[core], weight_ref.at[k * FF_DEV : (k + 1) * FF_DEV, :], sems.at[k]
        )
        for k, ref in enumerate((gate_hbm, got_gate_hbm, up_hbm, got_up_hbm))
    ]
    for copy in copies:
        copy.start()
    i, j = iota((LANES, LANES), 0), iota((LANES, LANES), 1)
    sort = (j == (i & (GROUP - 1)) * QUARTERS + (i >> 5)).astype(F32).astype(BF16)
    for g in range(NGROUPS):
        block = nn(sort, rows_ref[g * LANES : (g + 1) * LANES, :]).astype(BF16)
        for q in range(QUARTERS):
            x_ref[g * GROUP : (g + 1) * GROUP, q * QW : (q + 1) * QW] = block[
                q * GROUP : (q + 1) * GROUP, :
            ]
    for copy in copies:
        copy.wait()
    both = nt(x_ref[...], weight_ref[...])
    gate, upper = both[:, : 2 * FF_DEV], both[:, 2 * FF_DEV :]
    hidden = (gate / (1.0 + jnp.exp(-gate)) * upper).astype(BF16)
    for d in range(NY):
        out_ref[d] = hidden


def weigh_kernel(routes_ref, scores_ref, chi_ref, clo_ref):
    core = lax.axis_index("c")
    routes, scores = routes_ref[...], scores_ref[...]
    weights = scores / jnp.sum(scores, 0, keepdims=True) * 2.5
    weight = jnp.zeros((EXPERTS, TOK), F32)
    for k in range(TOPK):
        weight += jnp.where(
            routes[k : k + 1, :] == iota((EXPERTS, TOK), 0), weights[k : k + 1, :], 0.0
        )
    high = weight.astype(BF16)
    rest = weight - high.astype(F32)
    code = spread_tokens(membership(routes)).T.astype(BF16)
    high = spread_tokens(high).T.astype(BF16)
    rest = spread_tokens(rest).T.astype(BF16)
    expert, row = iota((EXPERTS, ROWS), 0), iota((EXPERTS, ROWS), 1)
    low = (expert - core) * (PIECE // 2)
    owner = ((expert & 1) == core) & (row >= low) & (row < low + PIECE)
    owner = owner.astype(F32).astype(BF16)
    found = nn(code, owner)
    token, row = iota((LANES, ROWS), 0), iota((LANES, ROWS), 1)
    table = (found == ((row >> 2) + 1).astype(F32)) & ((row & 3) == (token >> 5))
    table = table & ((token & (GROUP - 1)) < TOK)
    chi_ref[...] = jnp.where(table, nn(high, owner), 0.0).astype(BF16)
    clo_ref[...] = jnp.where(table, nn(rest, owner), 0.0).astype(BF16)


def down_kernel(hidden_ref, keep_ref, got_ref, out_ref, h_ref, stack_ref):
    for d in range(NY):
        h_ref[:, d * FF_DEV : (d + 1) * FF_DEV] = hidden_ref[d, :, :FF_DEV]
        h_ref[:, (NY + d) * FF_DEV : (NY + d + 1) * FF_DEV] = hidden_ref[d, :, FF_DEV:]
    wide = NY * FF_DEV
    done = (nn(h_ref[:, :wide], keep_ref[...]) + nn(h_ref[:, wide:], got_ref[...])).astype(BF16)
    for g in range(NGROUPS):
        for q in range(QUARTERS):
            stack_ref[g * LANES + q * GROUP : g * LANES + (q + 1) * GROUP, :] = done[
                g * GROUP : (g + 1) * GROUP, q * LANES : (q + 1) * LANES
            ]
    i, j = iota((LANES, LANES), 0), iota((LANES, LANES), 1)
    sort = (j == (i & 3) * GROUP + (i >> 2)).astype(F32).astype(BF16)
    for g in range(NGROUPS):
        rows = slice(g * LANES, (g + 1) * LANES)
        out_ref[rows, :] = nn(sort, stack_ref[rows, :]).astype(BF16)


def combine_kernel(rows_ref, chi_ref, clo_ref, shared_ref, mine_ref, other_ref, acc_ref):
    core = lax.axis_index("c")
    acc_ref[...] = nn(chi_ref[...], rows_ref[...]) + nn(clo_ref[...], rows_ref[...])
    per = HALF // LANES
    for half in range(NC):
        whole = jnp.concatenate(
            [
                acc_ref[q * GROUP : q * GROUP + TOK, :]
                + shared_ref[:, q * LANES : (q + 1) * LANES]
                for q in range(half * per, (half + 1) * per)
            ],
            axis=1,
        )

        @pl.when(core == half)
        def _():
            mine_ref[...] = whole

        @pl.when(core != half)
        def _():
            other_ref[...] = whole


def call(kernel, outs, scratch, flops, *args, specs=None, grant=24):
    return pl.pallas_call(
        kernel,
        out_shape=outs,
        in_specs=specs or [VM] * len(args),
        out_specs=jax.tree.map(lambda _: VM, outs),
        scratch_shapes=scratch,
        compiler_params=pltpu.CompilerParams(vmem_limit_bytes=grant << 20),
        cost_estimate=pl.CostEstimate(flops=flops, bytes_accessed=1 << 20, transcendentals=0),
    )(*args)


def out(shape, dtype=BF16):
    return jax.ShapeDtypeStruct(shape, dtype)


def hop(x, axis, size, step):
    return lax.ppermute(x, axis, [(i, (i + step) % size) for i in range(size)])


def body(
    tokens,
    norm_gain,
    routes,
    route_scores,
    expert_gate,
    expert_up,
    expert_down,
    shared_gate,
    shared_up,
    shared_down,
):
    send, normed = call(
        pack_kernel,
        (out((ROWS, QW)), out((TOK, D))),
        [
            pltpu.VMEM((LANES, QW), BF16),
            pltpu.VMEM((TOK, D), BF16),
            pltpu.VMEM((1, D), F32),
            pltpu.VMEM((TOPK, TOK), jnp.int32),
            pltpu.SemaphoreType.DMA((3,)),
        ],
        1 << 30,
        tokens,
        norm_gain.reshape(1, D),
        routes.T,
        specs=[HB] * 3,
        grant=62,
    )
    rows = lax.all_to_all(
        send.reshape(EP, PIECE, QW), ("z", "x"), split_axis=0, concat_axis=0, tiled=True
    ).reshape(ROWS, QW)
    messages = list(
        call(
            side_kernel,
            tuple(out((MSG, OUT_W)) for _ in range(NY)),
            [pltpu.VMEM((TOK, D), BF16)],
            1 << 30,
            normed,
            shared_gate,
            shared_up,
            shared_down,
            expert_down,
        )
    )
    for d in ORDER[1:]:
        messages[d] = hop(messages[d], "y", NY, d)
    got_gate, got_up = hop(expert_gate, "c", NC, 1), hop(expert_up, "c", NC, 1)
    chi, clo = call(
        weigh_kernel,
        (out((LANES, ROWS)), out((LANES, ROWS))),
        [],
        1 << 28,
        routes.T,
        route_scores.T,
    )
    wide = NY * FF_DEV
    keep, give, shared = call(
        ready_kernel,
        (out((wide, OUT_W)), out((wide, OUT_W)), out((TOK, OUT_W), F32)),
        [],
        1 << 28,
        *[messages[d] for d in ORDER],
    )
    got = hop(give, "c", NC, 1)
    hidden = call(
        hidden_kernel,
        out((NY, SLOTS, 2 * FF_DEV)),
        [
            pltpu.VMEM((SLOTS, D), BF16),
            pltpu.VMEM((4 * FF_DEV, D), BF16),
            pltpu.SemaphoreType.DMA((4,)),
        ],
        1 << 30,
        rows,
        expert_gate,
        got_gate,
        expert_up,
        got_up,
        shared,
        specs=[VM] + [HB] * 5,
        grant=60,
    )
    hidden = lax.all_to_all(hidden, "y", split_axis=0, concat_axis=0, tiled=True)
    back = call(
        down_kernel,
        out((ROWS, LANES)),
        [pltpu.VMEM((SLOTS, 2 * wide), BF16), pltpu.VMEM((ROWS, LANES), BF16)],
        1 << 30,
        hidden,
        keep,
        got,
    )
    back = lax.all_to_all(
        back.reshape(EP, PIECE, LANES), ("z", "x"), split_axis=0, concat_axis=0, tiled=True
    ).reshape(ROWS, LANES)
    mine, other = call(
        combine_kernel,
        (out((TOK, HALF), F32), out((TOK, HALF), F32)),
        [pltpu.VMEM((LANES, LANES), F32)],
        1 << 28,
        back,
        chi,
        clo,
        shared,
    )
    return (mine + hop(other, "c", NC, 1)).astype(BF16)


def solution(mesh):
    fine = Mesh(mesh.devices.reshape(NZ, NX, NY, NC), ("z", "x", "y", "c"))
    ep, tp = ("z", "x"), ("y", "c")
    in_specs = (
        P(ep, None),
        P(),
        P(ep, None),
        P(ep, None),
        P(ep, tp, None),
        P(ep, tp, None),
        P(ep, tp, None),
        P(tp, None),
        P(tp, None),
        P(tp, None),
    )
    return jax.shard_map(
        body, mesh=fine, in_specs=in_specs, out_specs=P(ep, tp), check_vma=False
    )
```

```python
import jax
import jax.numpy as jnp
from jax import lax
from jax.experimental import pallas as pl
from jax.experimental.pallas import tpu as pltpu
from jax.sharding import Mesh, PartitionSpec as P


NZ, NX, NY, NC = 8, 4, 8, 2
EP = NZ * NX
D = 4096
FF_DEV = 64
TOK = 24
TOPK = 6
EXPERTS = 64
CAP = 6
QUARTERS = 4
QW = D // QUARTERS
PIECE = CAP * QUARTERS
ROWS = EP * PIECE
SLOTS = EP * CAP
OUT_W = D // NY
HALF = OUT_W // NC
LANES = 128
GROUP = 32
NGROUPS = SLOTS // GROUP
MSG = NC * FF_DEV + TOK
ORDER = (0, 4, 5, 3, 6, 2, 7, 1)
BATCH = 8
PARTS = EP // BATCH
BACK = 16
BACK_ROWS = EXPERTS * BACK
VM = pl.BlockSpec(memory_space=pltpu.VMEM)
HB = pl.BlockSpec(memory_space=pltpu.HBM)
F32, BF16 = jnp.float32, jnp.bfloat16


def iota(shape, dim):
    return lax.broadcasted_iota(jnp.int32, shape, dim)


def nt(a, b):
    return lax.dot_general(a, b, (((1,), (1,)), ((), ())), preferred_element_type=F32)


def nn(a, b):
    return jnp.dot(a, b, preferred_element_type=F32)


def spread_tokens(values):
    lane, token = iota((TOK, LANES), 1), iota((TOK, LANES), 0)
    place = ((lane & (GROUP - 1)) == token).astype(F32).astype(BF16)
    return nn(values.astype(BF16), place)


def membership(routes, base):
    named = jnp.zeros((EXPERTS, TOK), F32)
    for k in range(TOPK):
        named += (routes[k : k + 1, :] == iota((EXPERTS, TOK), 0)).astype(F32)
    earlier = (iota((TOK, TOK), 0) < iota((TOK, TOK), 1)).astype(F32)
    rank = nn(named.astype(BF16), earlier.astype(BF16))
    return named * (rank + 1.0 + (base * (iota((EXPERTS, TOK), 0) >> 1)).astype(F32))


def pack_kernel(
    tok_hbm, gain_hbm, routes_hbm, send_ref, normed_ref, stack_ref, tok_ref, gain_ref, routes_ref, sems
):
    core = lax.axis_index("c")
    routes_copy = pltpu.make_async_copy(routes_hbm, routes_ref, sems.at[2])
    tok_copy = pltpu.make_async_copy(tok_hbm, tok_ref, sems.at[0])
    gain_copy = pltpu.make_async_copy(gain_hbm, gain_ref, sems.at[1])
    routes_copy.start()
    tok_copy.start()
    gain_copy.start()
    routes_copy.wait()
    code = spread_tokens(membership(routes_ref[...], CAP)).astype(BF16)
    row, expert = iota((ROWS, EXPERTS), 0), iota((ROWS, EXPERTS), 1)
    low = (expert - core) * (PIECE // 2)
    owner = ((expert & 1) == core) & (row >= low) & (row < low + PIECE)
    found = nn(owner.astype(F32).astype(BF16), code)
    row, col = iota((ROWS, LANES), 0), iota((ROWS, LANES), 1)
    table = (found == ((row >> 2) + 1).astype(F32)) & ((row & 3) == (col >> 5))
    table = table.astype(F32).astype(BF16)
    stack_ref[...] = jnp.zeros(stack_ref.shape, BF16)
    tok_copy.wait()
    gain_copy.wait()
    values = tok_ref[...].astype(F32)
    normed = (
        values * lax.rsqrt(jnp.mean(values * values, -1, keepdims=True) + 1e-06) * gain_ref[...]
    ).astype(BF16)
    normed_ref[...] = normed
    for q in range(QUARTERS):
        stack_ref[q * GROUP : q * GROUP + TOK, :] = normed[:, q * QW : (q + 1) * QW]
    chunk = ROWS // 4
    for k in range(4):
        send_ref[k * chunk : (k + 1) * chunk, :] = nn(
            table[k * chunk : (k + 1) * chunk, :], stack_ref[...]
        ).astype(BF16)


def side_kernel(normed_ref, sg_ref, su_ref, sd_ref, down_ref, *refs):
    messages, part_ref = refs[:NY], refs[NY]
    me = lax.axis_index("y")
    normed = normed_ref[...]
    gate, upper = nt(normed, sg_ref[...]), nt(normed, su_ref[...])
    hidden = (gate / (1.0 + jnp.exp(-gate)) * upper).astype(BF16)
    part_ref[...] = nn(hidden, sd_ref[...]).astype(BF16)
    for d in range(NY):
        cols = pl.ds(pl.multiple_of(lax.rem(me + d, NY) * OUT_W, OUT_W), OUT_W)
        messages[d][0:FF_DEV, :] = down_ref[0, :, cols]
        messages[d][FF_DEV : 2 * FF_DEV, :] = down_ref[1, :, cols]
        messages[d][2 * FF_DEV : MSG, :] = part_ref[:, cols]


def ready_kernel(*refs):
    messages, (keep_ref, give_ref, mine_ref, other_ref) = dict(zip(ORDER, refs)), refs[NY:]
    core, me = lax.axis_index("c"), lax.axis_index("y")
    shared = jnp.zeros((TOK, OUT_W), F32)
    for d in range(NY):
        source = lax.rem(me + NY - d, NY)
        rows = pl.ds(pl.multiple_of(source * FF_DEV, FF_DEV), FF_DEV)
        keep_ref[rows, :] = messages[d][pl.ds(pl.multiple_of(core * FF_DEV, FF_DEV), FF_DEV), :]
        give_ref[rows, :] = messages[d][
            pl.ds(pl.multiple_of((1 - core) * FF_DEV, FF_DEV), FF_DEV), :
        ]
        shared += messages[d][2 * FF_DEV : MSG, :].astype(F32)
    for half in range(NC):

        @pl.when(core == half)
        def _():
            mine_ref[...] = shared[:, half * HALF : (half + 1) * HALF]

        @pl.when(core != half)
        def _():
            other_ref[...] = shared[:, half * HALF : (half + 1) * HALF]


def hidden_kernel(
    rows_hbm,
    gate_hbm,
    got_gate_hbm,
    up_hbm,
    got_up_hbm,
    after_ref,
    out_ref,
    rows_ref,
    x_ref,
    weight_ref,
    row_sems,
    sems,
):
    core = lax.axis_index("c")
    pieces = [
        pltpu.make_async_copy(
            rows_hbm.at[g * LANES : (g + 1) * LANES, :],
            rows_ref.at[g * LANES : (g + 1) * LANES, :],
            row_sems.at[g],
        )
        for g in range(NGROUPS)
    ]
    copies = [
        pltpu.make_async_copy(
            ref.at[core], weight_ref.at[k * FF_DEV : (k + 1) * FF_DEV, :], sems.at[k]
        )
        for k, ref in enumerate((gate_hbm, got_gate_hbm, up_hbm, got_up_hbm))
    ]
    for copy in pieces + copies:
        copy.start()
    i, j = iota((LANES, LANES), 0), iota((LANES, LANES), 1)
    sort = (j == (i & (GROUP - 1)) * QUARTERS + (i >> 5)).astype(F32).astype(BF16)
    for g in range(NGROUPS):
        pieces[g].wait()
        block = nn(sort, rows_ref[g * LANES : (g + 1) * LANES, :]).astype(BF16)
        for q in range(QUARTERS):
            x_ref[g * GROUP : (g + 1) * GROUP, q * QW : (q + 1) * QW] = block[
                q * GROUP : (q + 1) * GROUP, :
            ]
    for copy in copies:
        copy.wait()
    both = nt(x_ref[...], weight_ref[...])
    gate, upper = both[:, : 2 * FF_DEV], both[:, 2 * FF_DEV :]
    hidden = (gate / (1.0 + jnp.exp(-gate)) * upper).astype(BF16)
    for d in range(NY):
        out_ref[d] = hidden


def weigh_kernel(routes_ref, scores_ref, chi_ref, clo_ref):
    routes, scores = routes_ref[...], scores_ref[...]
    weights = scores / jnp.sum(scores, 0, keepdims=True) * 2.5
    weight = jnp.zeros((EXPERTS, TOK), F32)
    for k in range(TOPK):
        weight += jnp.where(
            routes[k : k + 1, :] == iota((EXPERTS, TOK), 0), weights[k : k + 1, :], 0.0
        )
    high = weight.astype(BF16)
    rest = weight - high.astype(F32)
    rank = membership(routes, 0)
    half = NC * GROUP
    code = spread_tokens(rank).T[:half].astype(BF16)
    high = spread_tokens(high).T[:half].astype(BF16)
    rest = spread_tokens(rest).T[:half].astype(BF16)
    shape = (EXPERTS, BACK_ROWS)
    owner = ((iota(shape, 1) >> 4) == iota(shape, 0)).astype(F32).astype(BF16)
    found = nn(code, owner)
    token, row = iota((half, BACK_ROWS), 0), iota((half, BACK_ROWS), 1)
    table = (found == (((row >> 1) & 7) + 1).astype(F32)) & ((row & 1) == (token >> 5))
    chi_ref[...] = jnp.where(table, nn(high, owner), 0.0).astype(BF16)
    clo_ref[...] = jnp.where(table, nn(rest, owner), 0.0).astype(BF16)


def down_kernel(hidden_ref, keep_ref, got_ref, out_ref, h_ref, stack_ref):
    for d in range(NY):
        h_ref[:, d * FF_DEV : (d + 1) * FF_DEV] = hidden_ref[d, :, :FF_DEV]
        h_ref[:, (NY + d) * FF_DEV : (NY + d + 1) * FF_DEV] = hidden_ref[d, :, FF_DEV:]
    wide = NY * FF_DEV
    done = (nn(h_ref[:, :wide], keep_ref[...]) + nn(h_ref[:, wide:], got_ref[...])).astype(BF16)
    slots = BATCH * CAP
    for p in range(PARTS):
        for q in range(QUARTERS):
            stack_ref[(p * QUARTERS + q) * slots : (p * QUARTERS + q + 1) * slots, :] = done[
                p * slots : (p + 1) * slots, q * LANES : (q + 1) * LANES
            ]
    shape = (BATCH * NC * BACK, QUARTERS * slots)
    i, j = iota(shape, 0), iota(shape, 1)
    slot = (i >> 1) & 7
    quarter = ((i >> 4) & 1) * 2 + (i & 1)
    place = (j == quarter * slots + (i >> 5) * CAP + slot) & (slot < CAP)
    place = place.astype(F32).astype(BF16)
    for p in range(PARTS):
        out_ref[p * shape[0] : (p + 1) * shape[0], :] = nn(
            place, stack_ref[p * shape[1] : (p + 1) * shape[1], :]
        ).astype(BF16)


def combine_kernel(rows_ref, chi_ref, clo_ref, mine_ref, got_ref, out_ref):
    total = nn(chi_ref[...], rows_ref[...]) + nn(clo_ref[...], rows_ref[...])
    for q in range(NC):
        cols = slice(q * LANES, (q + 1) * LANES)
        out_ref[:, cols] = (
            total[q * GROUP : q * GROUP + TOK, :] + (mine_ref[:, cols] + got_ref[:, cols])
        ).astype(BF16)


def call(kernel, outs, scratch, flops, *args, specs=None, grant=24):
    return pl.pallas_call(
        kernel,
        out_shape=outs,
        in_specs=specs or [VM] * len(args),
        out_specs=jax.tree.map(lambda _: VM, outs),
        scratch_shapes=scratch,
        compiler_params=pltpu.CompilerParams(vmem_limit_bytes=grant << 20),
        cost_estimate=pl.CostEstimate(flops=flops, bytes_accessed=1 << 20, transcendentals=0),
    )(*args)


def out(shape, dtype=BF16):
    return jax.ShapeDtypeStruct(shape, dtype)


def hop(x, axis, size, step):
    return lax.ppermute(x, axis, [(i, (i + step) % size) for i in range(size)])


def body(
    tokens,
    norm_gain,
    routes,
    route_scores,
    expert_gate,
    expert_up,
    expert_down,
    shared_gate,
    shared_up,
    shared_down,
):
    send, normed = call(
        pack_kernel,
        (out((ROWS, QW)), out((TOK, D))),
        [
            pltpu.VMEM((LANES, QW), BF16),
            pltpu.VMEM((TOK, D), BF16),
            pltpu.VMEM((1, D), F32),
            pltpu.VMEM((TOPK, TOK), jnp.int32),
            pltpu.SemaphoreType.DMA((3,)),
        ],
        1 << 30,
        tokens,
        norm_gain.reshape(1, D),
        routes.T,
        specs=[HB] * 3,
        grant=62,
    )
    rows = lax.all_to_all(
        send.reshape(EP, PIECE, QW), ("z", "x"), split_axis=0, concat_axis=0, tiled=True
    ).reshape(ROWS, QW)
    messages = list(
        call(
            side_kernel,
            tuple(out((MSG, OUT_W)) for _ in range(NY)),
            [pltpu.VMEM((TOK, D), BF16)],
            1 << 30,
            normed,
            shared_gate,
            shared_up,
            shared_down,
            expert_down,
        )
    )
    for d in ORDER[1:]:
        messages[d] = hop(messages[d], "y", NY, d)
    got_gate = hop(expert_gate, "c", NC, 1)
    got_up = hop(expert_up, "c", NC, 1)
    chi, clo = call(
        weigh_kernel,
        (out((NC * GROUP, BACK_ROWS)), out((NC * GROUP, BACK_ROWS))),
        [],
        1 << 28,
        routes.T,
        route_scores.T,
    )
    wide = NY * FF_DEV
    keep, give, mine, other = call(
        ready_kernel,
        (out((wide, OUT_W)), out((wide, OUT_W)), out((TOK, HALF), F32), out((TOK, HALF), F32)),
        [],
        1 << 28,
        *[messages[d] for d in ORDER],
    )
    got, other = hop(give, "c", NC, 1), hop(other, "c", NC, 1)
    hidden = call(
        hidden_kernel,
        out((NY, SLOTS, 2 * FF_DEV)),
        [
            pltpu.VMEM((ROWS, QW), BF16),
            pltpu.VMEM((SLOTS, D), BF16),
            pltpu.VMEM((4 * FF_DEV, D), BF16),
            pltpu.SemaphoreType.DMA((NGROUPS,)),
            pltpu.SemaphoreType.DMA((4,)),
        ],
        1 << 30,
        rows,
        expert_gate,
        got_gate,
        expert_up,
        got_up,
        mine,
        specs=[HB] * 5 + [VM],
        grant=60,
    )
    hidden = lax.all_to_all(hidden, "y", split_axis=0, concat_axis=0, tiled=True)
    back = call(
        down_kernel,
        out((BACK_ROWS, LANES)),
        [pltpu.VMEM((SLOTS, 2 * wide), BF16), pltpu.VMEM((QUARTERS * SLOTS, LANES), BF16)],
        1 << 30,
        hidden,
        keep,
        got,
    )
    back = lax.all_to_all(
        back.reshape(EXPERTS, BACK, LANES), ("z", "x", "c"), split_axis=0, concat_axis=0, tiled=True
    ).reshape(BACK_ROWS, LANES)
    return call(combine_kernel, out((TOK, HALF)), [], 1 << 28, back, chi, clo, mine, other)


def solution(mesh):
    fine = Mesh(mesh.devices.reshape(NZ, NX, NY, NC), ("z", "x", "y", "c"))
    ep, tp = ("z", "x"), ("y", "c")
    in_specs = (
        P(ep, None),
        P(),
        P(ep, None),
        P(ep, None),
        P(ep, tp, None),
        P(ep, tp, None),
        P(ep, tp, None),
        P(tp, None),
        P(tp, None),
        P(tp, None),
    )
    return jax.shard_map(body, mesh=fine, in_specs=in_specs, out_specs=P(ep, tp), check_vma=False)
```

```python
import jax
import jax.numpy as jnp
from jax import lax
from jax.experimental import pallas as pl
from jax.experimental.pallas import tpu as pltpu
from jax.sharding import Mesh, PartitionSpec as P


NZ, NX, NY, NC = 8, 4, 8, 2
EP = NZ * NX
D = 4096
FF_DEV = 64
TOK = 24
TOPK = 6
EXPERTS = 64
CAP = 6
QUARTERS = 4
QW = D // QUARTERS
PIECE = CAP * QUARTERS
ROWS = EP * PIECE
SLOTS = EP * CAP
OUT_W = D // NY
HALF = OUT_W // NC
LANES = 128
GROUP = 32
NGROUPS = SLOTS // GROUP
MSG = NC * FF_DEV + TOK
ORDER = (0, 4, 5, 3, 6, 2, 7, 1)
SENDS = 4
LOADS = 3
BATCH = 8
PARTS = EP // BATCH
BACK = 16
BACK_ROWS = EXPERTS * BACK
VM = pl.BlockSpec(memory_space=pltpu.VMEM)
HB = pl.BlockSpec(memory_space=pltpu.HBM)
F32, BF16 = jnp.float32, jnp.bfloat16


def iota(shape, dim):
    return lax.broadcasted_iota(jnp.int32, shape, dim)


def nt(a, b):
    return lax.dot_general(a, b, (((1,), (1,)), ((), ())), preferred_element_type=F32)


def nn(a, b):
    return jnp.dot(a, b, preferred_element_type=F32)


def spread_tokens(values):
    lane, token = iota((TOK, LANES), 1), iota((TOK, LANES), 0)
    place = ((lane & (GROUP - 1)) == token).astype(F32).astype(BF16)
    return nn(values.astype(BF16), place)


def membership(routes, base):
    named = jnp.zeros((EXPERTS, TOK), F32)
    for k in range(TOPK):
        named += (routes[k : k + 1, :] == iota((EXPERTS, TOK), 0)).astype(F32)
    earlier = (iota((TOK, TOK), 0) < iota((TOK, TOK), 1)).astype(F32)
    rank = nn(named.astype(BF16), earlier.astype(BF16))
    return named * (rank + 1.0 + (base * (iota((EXPERTS, TOK), 0) >> 1)).astype(F32))


def pack_kernel(
    tok_hbm,
    gain_hbm,
    routes_hbm,
    send_hbm,
    normed_hbm,
    stack_ref,
    tok_ref,
    gain_ref,
    routes_ref,
    send_ref,
    normed_ref,
    sems,
    out_sems,
):
    core = lax.axis_index("c")
    routes_copy = pltpu.make_async_copy(routes_hbm, routes_ref, sems.at[2])
    tok_copy = pltpu.make_async_copy(tok_hbm, tok_ref, sems.at[0])
    gain_copy = pltpu.make_async_copy(gain_hbm, gain_ref, sems.at[1])
    routes_copy.start()
    tok_copy.start()
    gain_copy.start()
    stack_ref[...] = jnp.zeros(stack_ref.shape, BF16)
    row, expert = iota((ROWS, EXPERTS), 0), iota((ROWS, EXPERTS), 1)
    low = (expert - core) * (PIECE // 2)
    owner = ((expert & 1) == core) & (row >= low) & (row < low + PIECE)
    owner = owner.astype(F32).astype(BF16)
    routes_copy.wait()
    code = spread_tokens(membership(routes_ref[...], CAP)).astype(BF16)
    found = nn(owner, code)
    row, col = iota((ROWS, LANES), 0), iota((ROWS, LANES), 1)
    table = (found == ((row >> 2) + 1).astype(F32)) & ((row & 3) == (col >> 5))
    table = table.astype(F32).astype(BF16)
    tok_copy.wait()
    gain_copy.wait()
    values = tok_ref[...].astype(F32)
    normed = (
        values * lax.rsqrt(jnp.mean(values * values, -1, keepdims=True) + 1e-06) * gain_ref[...]
    ).astype(BF16)
    normed_ref[...] = normed
    for q in range(QUARTERS):
        stack_ref[q * GROUP : q * GROUP + TOK, :] = normed[:, q * QW : (q + 1) * QW]
    chunk = ROWS // SENDS
    copies = []
    for k in range(SENDS):
        rows = slice(k * chunk, (k + 1) * chunk)
        send_ref[rows, :] = nn(table[rows, :], stack_ref[...]).astype(BF16)
        copies.append(
            pltpu.make_async_copy(send_ref.at[rows, :], send_hbm.at[rows, :], out_sems.at[k])
        )
        copies[k].start()
    copies.append(pltpu.make_async_copy(normed_ref, normed_hbm, out_sems.at[SENDS]))
    copies[SENDS].start()
    for copy in copies:
        copy.wait()


def side_kernel(normed_ref, sg_ref, su_ref, sd_ref, down_ref, gate_hbm, up_hbm, *refs):
    messages, (swap_ref, part_ref, sems) = refs[:NY], refs[NY:]
    core, me = lax.axis_index("c"), lax.axis_index("y")
    copies = [
        pltpu.make_async_copy(
            ref.at[1 - core], swap_ref.at[k * FF_DEV : (k + 1) * FF_DEV, :], sems.at[k]
        )
        for k, ref in enumerate((gate_hbm, up_hbm))
    ]
    for copy in copies:
        copy.start()
    normed = normed_ref[...]
    gate, upper = nt(normed, sg_ref[...]), nt(normed, su_ref[...])
    hidden = (gate / (1.0 + jnp.exp(-gate)) * upper).astype(BF16)
    part_ref[...] = nn(hidden, sd_ref[...]).astype(BF16)
    for d in range(NY):
        cols = pl.ds(pl.multiple_of(lax.rem(me + d, NY) * OUT_W, OUT_W), OUT_W)
        messages[d][0:FF_DEV, :] = down_ref[0, :, cols]
        messages[d][FF_DEV : 2 * FF_DEV, :] = down_ref[1, :, cols]
        messages[d][2 * FF_DEV : MSG, :] = part_ref[:, cols]
    for copy in copies:
        copy.wait()


def ready_kernel(*refs):
    messages = dict(zip(ORDER, refs))
    keep_ref, give_ref, mine_ref, other_ref, flag_ref = refs[NY:]
    core, me = lax.axis_index("c"), lax.axis_index("y")
    flag_ref[...] = jnp.zeros(flag_ref.shape, F32)
    shared = jnp.zeros((TOK, OUT_W), F32)
    for d in range(NY):
        source = lax.rem(me + NY - d, NY)
        rows = pl.ds(pl.multiple_of(source * FF_DEV, FF_DEV), FF_DEV)
        keep_ref[rows, :] = messages[d][pl.ds(pl.multiple_of(core * FF_DEV, FF_DEV), FF_DEV), :]
        give_ref[rows, :] = messages[d][
            pl.ds(pl.multiple_of((1 - core) * FF_DEV, FF_DEV), FF_DEV), :
        ]
        shared += messages[d][2 * FF_DEV : MSG, :].astype(F32)
    for half in range(NC):

        @pl.when(core == half)
        def _():
            mine_ref[...] = shared[:, half * HALF : (half + 1) * HALF]

        @pl.when(core != half)
        def _():
            other_ref[...] = shared[:, half * HALF : (half + 1) * HALF]


def hidden_kernel(
    rows_hbm, gate_hbm, up_hbm, got_hbm, flag_ref, out_ref, rows_ref, x_ref, weight_ref, row_sems, sems
):
    core = lax.axis_index("c")
    size = ROWS // LOADS
    pieces = [
        pltpu.make_async_copy(
            rows_hbm.at[k * size : (k + 1) * size, :],
            rows_ref.at[k * size : (k + 1) * size, :],
            row_sems.at[k],
        )
        for k in range(LOADS)
    ]
    sources = (
        gate_hbm.at[core],
        got_hbm.at[0:FF_DEV],
        up_hbm.at[core],
        got_hbm.at[FF_DEV : 2 * FF_DEV],
    )
    copies = [
        pltpu.make_async_copy(ref, weight_ref.at[k * FF_DEV : (k + 1) * FF_DEV, :], sems.at[k])
        for k, ref in enumerate(sources)
    ]
    for copy in pieces + copies:
        copy.start()
    i, j = iota((LANES, LANES), 0), iota((LANES, LANES), 1)
    sort = (j == (i & (GROUP - 1)) * QUARTERS + (i >> 5)).astype(F32).astype(BF16)
    for g in range(NGROUPS):
        if g * LANES % size == 0:
            pieces[g * LANES // size].wait()
        block = nn(sort, rows_ref[g * LANES : (g + 1) * LANES, :]).astype(BF16)
        for q in range(QUARTERS):
            x_ref[g * GROUP : (g + 1) * GROUP, q * QW : (q + 1) * QW] = block[
                q * GROUP : (q + 1) * GROUP, :
            ]
    for copy in copies:
        copy.wait()
    both = nt(x_ref[...], weight_ref[...])
    gate, upper = both[:, : 2 * FF_DEV], both[:, 2 * FF_DEV :]
    hidden = (gate / (1.0 + jnp.exp(-gate)) * upper).astype(BF16)
    for d in range(NY):
        out_ref[d] = hidden


def weigh_kernel(routes_ref, scores_ref, chi_ref, clo_ref):
    routes, scores = routes_ref[...], scores_ref[...]
    weights = scores / jnp.sum(scores, 0, keepdims=True) * 2.5
    weight = jnp.zeros((EXPERTS, TOK), F32)
    for k in range(TOPK):
        weight += jnp.where(
            routes[k : k + 1, :] == iota((EXPERTS, TOK), 0), weights[k : k + 1, :], 0.0
        )
    high = weight.astype(BF16)
    rest = weight - high.astype(F32)
    rank = membership(routes, 0)
    half = NC * GROUP
    code = spread_tokens(rank).T[:half].astype(BF16)
    high = spread_tokens(high).T[:half].astype(BF16)
    rest = spread_tokens(rest).T[:half].astype(BF16)
    shape = (EXPERTS, BACK_ROWS)
    owner = ((iota(shape, 1) >> 4) == iota(shape, 0)).astype(F32).astype(BF16)
    found = nn(code, owner)
    token, row = iota((half, BACK_ROWS), 0), iota((half, BACK_ROWS), 1)
    table = (found == (((row >> 1) & 7) + 1).astype(F32)) & ((row & 1) == (token >> 5))
    chi_ref[...] = jnp.where(table, nn(high, owner), 0.0).astype(BF16)
    clo_ref[...] = jnp.where(table, nn(rest, owner), 0.0).astype(BF16)


def down_kernel(hidden_ref, keep_ref, got_ref, out_ref, h_ref, stack_ref):
    for d in range(NY):
        h_ref[:, d * FF_DEV : (d + 1) * FF_DEV] = hidden_ref[d, :, :FF_DEV]
        h_ref[:, (NY + d) * FF_DEV : (NY + d + 1) * FF_DEV] = hidden_ref[d, :, FF_DEV:]
    wide = NY * FF_DEV
    done = (nn(h_ref[:, :wide], keep_ref[...]) + nn(h_ref[:, wide:], got_ref[...])).astype(BF16)
    slots = BATCH * CAP
    for p in range(PARTS):
        for q in range(QUARTERS):
            stack_ref[(p * QUARTERS + q) * slots : (p * QUARTERS + q + 1) * slots, :] = done[
                p * slots : (p + 1) * slots, q * LANES : (q + 1) * LANES
            ]
    shape = (BATCH * NC * BACK, QUARTERS * slots)
    i, j = iota(shape, 0), iota(shape, 1)
    slot = (i >> 1) & 7
    quarter = ((i >> 4) & 1) * 2 + (i & 1)
    place = (j == quarter * slots + (i >> 5) * CAP + slot) & (slot < CAP)
    place = place.astype(F32).astype(BF16)
    for p in range(PARTS):
        out_ref[p * shape[0] : (p + 1) * shape[0], :] = nn(
            place, stack_ref[p * shape[1] : (p + 1) * shape[1], :]
        ).astype(BF16)


def combine_kernel(rows_ref, chi_ref, clo_ref, mine_ref, got_ref, out_ref):
    total = nn(chi_ref[...], rows_ref[...]) + nn(clo_ref[...], rows_ref[...])
    for q in range(NC):
        cols = slice(q * LANES, (q + 1) * LANES)
        out_ref[:, cols] = (
            total[q * GROUP : q * GROUP + TOK, :] + (mine_ref[:, cols] + got_ref[:, cols])
        ).astype(BF16)


def call(kernel, outs, scratch, flops, *args, specs=None, out_specs=None, grant=24):
    return pl.pallas_call(
        kernel,
        out_shape=outs,
        in_specs=specs or [VM] * len(args),
        out_specs=out_specs or jax.tree.map(lambda _: VM, outs),
        scratch_shapes=scratch,
        compiler_params=pltpu.CompilerParams(vmem_limit_bytes=grant << 20),
        cost_estimate=pl.CostEstimate(flops=flops, bytes_accessed=1 << 20, transcendentals=0),
    )(*args)


def out(shape, dtype=BF16):
    return jax.ShapeDtypeStruct(shape, dtype)


def hop(x, axis, size, step):
    return lax.ppermute(x, axis, [(i, (i + step) % size) for i in range(size)])


def body(
    tokens,
    norm_gain,
    routes,
    route_scores,
    expert_gate,
    expert_up,
    expert_down,
    shared_gate,
    shared_up,
    shared_down,
):
    send, normed = call(
        pack_kernel,
        (out((ROWS, QW)), out((TOK, D))),
        [
            pltpu.VMEM((LANES, QW), BF16),
            pltpu.VMEM((TOK, D), BF16),
            pltpu.VMEM((1, D), F32),
            pltpu.VMEM((TOPK, TOK), jnp.int32),
            pltpu.VMEM((ROWS, QW), BF16),
            pltpu.VMEM((TOK, D), BF16),
            pltpu.SemaphoreType.DMA((3,)),
            pltpu.SemaphoreType.DMA((SENDS + 1,)),
        ],
        1 << 30,
        tokens,
        norm_gain.reshape(1, D),
        routes.T,
        specs=[HB] * 3,
        out_specs=(HB, HB),
        grant=62,
    )
    rows = lax.all_to_all(
        send.reshape(EP, PIECE, QW), ("z", "x"), split_axis=0, concat_axis=0, tiled=True
    ).reshape(ROWS, QW)
    *messages, swap = call(
        side_kernel,
        tuple(out((MSG, OUT_W)) for _ in range(NY)) + (out((2 * FF_DEV, D)),),
        [pltpu.VMEM((TOK, D), BF16), pltpu.SemaphoreType.DMA((2,))],
        1 << 30,
        normed,
        shared_gate,
        shared_up,
        shared_down,
        expert_down,
        expert_gate,
        expert_up,
        specs=[VM] * 5 + [HB] * 2,
    )
    for d in ORDER[1:]:
        messages[d] = hop(messages[d], "y", NY, d)
    swapped = hop(swap, "c", NC, 1)
    chi, clo = call(
        weigh_kernel,
        (out((NC * GROUP, BACK_ROWS)), out((NC * GROUP, BACK_ROWS))),
        [],
        1 << 28,
        routes.T,
        route_scores.T,
    )
    wide = NY * FF_DEV
    keep, give, mine, other, flag = call(
        ready_kernel,
        (
            out((wide, OUT_W)),
            out((wide, OUT_W)),
            out((TOK, HALF), F32),
            out((TOK, HALF), F32),
            out((8, LANES), F32),
        ),
        [],
        1 << 28,
        *[messages[d] for d in ORDER],
    )
    got, other = hop(give, "c", NC, 1), hop(other, "c", NC, 1)
    hidden = call(
        hidden_kernel,
        out((NY, SLOTS, 2 * FF_DEV)),
        [
            pltpu.VMEM((ROWS, QW), BF16),
            pltpu.VMEM((SLOTS, D), BF16),
            pltpu.VMEM((4 * FF_DEV, D), BF16),
            pltpu.SemaphoreType.DMA((LOADS,)),
            pltpu.SemaphoreType.DMA((4,)),
        ],
        1 << 30,
        rows,
        expert_gate,
        expert_up,
        swapped,
        flag,
        specs=[HB] * 4 + [VM],
        grant=52,
    )
    hidden = lax.all_to_all(hidden, "y", split_axis=0, concat_axis=0, tiled=True)
    back = call(
        down_kernel,
        out((BACK_ROWS, LANES)),
        [pltpu.VMEM((SLOTS, 2 * wide), BF16), pltpu.VMEM((QUARTERS * SLOTS, LANES), BF16)],
        1 << 30,
        hidden,
        keep,
        got,
    )
    back = lax.all_to_all(
        back.reshape(EXPERTS, BACK, LANES), ("z", "x", "c"), split_axis=0, concat_axis=0, tiled=True
    ).reshape(BACK_ROWS, LANES)
    return call(combine_kernel, out((TOK, HALF)), [], 1 << 28, back, chi, clo, mine, other)


def solution(mesh):
    fine = Mesh(mesh.devices.reshape(NZ, NX, NY, NC), ("z", "x", "y", "c"))
    ep, tp = ("z", "x"), ("y", "c")
    in_specs = (
        P(ep, None),
        P(),
        P(ep, None),
        P(ep, None),
        P(ep, tp, None),
        P(ep, tp, None),
        P(ep, tp, None),
        P(tp, None),
        P(tp, None),
        P(tp, None),
    )
    return jax.shard_map(body, mesh=fine, in_specs=in_specs, out_specs=P(ep, tp), check_vma=False)
```

```python
import jax
import jax.numpy as jnp
from jax import lax
from jax.experimental import pallas as pl
from jax.experimental.pallas import tpu as pltpu
from jax.sharding import Mesh, PartitionSpec as P


NZ, NX, NY, NC = 8, 4, 8, 2
EP = NZ * NX
D = 4096
FF_DEV = 64
TOK = 24
TOPK = 6
EXPERTS = 64
CAP = 6
QUARTERS = 4
QW = D // QUARTERS
PIECE = CAP * QUARTERS
ROWS = EP * PIECE
SLOTS = EP * CAP
OUT_W = D // NY
HALF = OUT_W // NC
LANES = 128
GROUP = 32
NGROUPS = SLOTS // GROUP
MSG = NC * FF_DEV + TOK
ORDER = (0, 4, 5, 3, 6, 2, 7, 1)
SENDS = 4
LOADS = 3
BATCH = 8
PARTS = EP // BATCH
BACK = 16
BACK_ROWS = EXPERTS * BACK
VM = pl.BlockSpec(memory_space=pltpu.VMEM)
HB = pl.BlockSpec(memory_space=pltpu.HBM)
F32, BF16 = jnp.float32, jnp.bfloat16


def iota(shape, dim):
    return lax.broadcasted_iota(jnp.int32, shape, dim)


def nt(a, b):
    return lax.dot_general(a, b, (((1,), (1,)), ((), ())), preferred_element_type=F32)


def nn(a, b):
    return jnp.dot(a, b, preferred_element_type=F32)


def spread_tokens(values):
    lane, token = iota((TOK, LANES), 1), iota((TOK, LANES), 0)
    place = ((lane & (GROUP - 1)) == token).astype(F32).astype(BF16)
    return nn(values.astype(BF16), place)


def membership(routes, base):
    named = jnp.zeros((EXPERTS, TOK), F32)
    for k in range(TOPK):
        named += (routes[k : k + 1, :] == iota((EXPERTS, TOK), 0)).astype(F32)
    earlier = (iota((TOK, TOK), 0) < iota((TOK, TOK), 1)).astype(F32)
    rank = nn(named.astype(BF16), earlier.astype(BF16))
    return named * (rank + 1.0 + (base * (iota((EXPERTS, TOK), 0) >> 1)).astype(F32))


def pack_kernel(
    tok_hbm,
    gain_hbm,
    routes_hbm,
    send_hbm,
    normed_hbm,
    stack_ref,
    tok_ref,
    gain_ref,
    routes_ref,
    send_ref,
    normed_ref,
    sems,
    out_sems,
):
    core = lax.axis_index("c")
    routes_copy = pltpu.make_async_copy(routes_hbm, routes_ref, sems.at[2])
    tok_copy = pltpu.make_async_copy(tok_hbm, tok_ref, sems.at[0])
    gain_copy = pltpu.make_async_copy(gain_hbm, gain_ref, sems.at[1])
    routes_copy.start()
    tok_copy.start()
    gain_copy.start()
    stack_ref[...] = jnp.zeros(stack_ref.shape, BF16)
    row, expert = iota((ROWS, EXPERTS), 0), iota((ROWS, EXPERTS), 1)
    low = (expert - core) * (PIECE // 2)
    owner = ((expert & 1) == core) & (row >= low) & (row < low + PIECE)
    owner = owner.astype(F32).astype(BF16)
    routes_copy.wait()
    code = spread_tokens(membership(routes_ref[...], CAP)).astype(BF16)
    found = nn(owner, code)
    row, col = iota((ROWS, LANES), 0), iota((ROWS, LANES), 1)
    table = (found == ((row >> 2) + 1).astype(F32)) & ((row & 3) == (col >> 5))
    table = table.astype(F32).astype(BF16)
    tok_copy.wait()
    gain_copy.wait()
    values = tok_ref[...].astype(F32)
    normed = (
        values * lax.rsqrt(jnp.mean(values * values, -1, keepdims=True) + 1e-06) * gain_ref[...]
    ).astype(BF16)
    normed_ref[...] = normed
    for q in range(QUARTERS):
        stack_ref[q * GROUP : q * GROUP + TOK, :] = normed[:, q * QW : (q + 1) * QW]
    chunk = ROWS // SENDS
    copies = []
    for k in range(SENDS):
        rows = slice(k * chunk, (k + 1) * chunk)
        send_ref[rows, :] = nn(table[rows, :], stack_ref[...]).astype(BF16)
        copies.append(
            pltpu.make_async_copy(send_ref.at[rows, :], send_hbm.at[rows, :], out_sems.at[k])
        )
        copies[k].start()
    copies.append(pltpu.make_async_copy(normed_ref, normed_hbm, out_sems.at[SENDS]))
    copies[SENDS].start()
    for copy in copies:
        copy.wait()


def side_kernel(normed_ref, sg_ref, su_ref, sd_ref, down_ref, *refs):
    messages, part_ref = refs[:NY], refs[NY]
    me = lax.axis_index("y")
    normed = normed_ref[...]
    gate, upper = nt(normed, sg_ref[...]), nt(normed, su_ref[...])
    hidden = (gate / (1.0 + jnp.exp(-gate)) * upper).astype(BF16)
    part_ref[...] = nn(hidden, sd_ref[...]).astype(BF16)
    for d in range(NY):
        cols = pl.ds(pl.multiple_of(lax.rem(me + d, NY) * OUT_W, OUT_W), OUT_W)
        messages[d][0:FF_DEV, :] = down_ref[0, :, cols]
        messages[d][FF_DEV : 2 * FF_DEV, :] = down_ref[1, :, cols]
        messages[d][2 * FF_DEV : MSG, :] = part_ref[:, cols]


def ready_kernel(*refs):
    messages = dict(zip(ORDER, refs))
    keep_ref, give_ref, mine_ref, other_ref = refs[NY:]
    core, me = lax.axis_index("c"), lax.axis_index("y")
    shared = jnp.zeros((TOK, OUT_W), F32)
    for d in range(NY):
        source = lax.rem(me + NY - d, NY)
        rows = pl.ds(pl.multiple_of(source * FF_DEV, FF_DEV), FF_DEV)
        keep_ref[rows, :] = messages[d][pl.ds(pl.multiple_of(core * FF_DEV, FF_DEV), FF_DEV), :]
        give_ref[rows, :] = messages[d][
            pl.ds(pl.multiple_of((1 - core) * FF_DEV, FF_DEV), FF_DEV), :
        ]
        shared += messages[d][2 * FF_DEV : MSG, :].astype(F32)
    for half in range(NC):

        @pl.when(core == half)
        def _():
            mine_ref[...] = shared[:, half * HALF : (half + 1) * HALF]

        @pl.when(core != half)
        def _():
            other_ref[...] = shared[:, half * HALF : (half + 1) * HALF]


def hidden_kernel(
    rows_hbm, gate_hbm, got_gate_hbm, up_hbm, got_up_hbm, after_hbm, out_ref, rows_ref, x_ref, weight_ref, row_sems, sems
):
    core = lax.axis_index("c")
    size = ROWS // LOADS
    pieces = [
        pltpu.make_async_copy(
            rows_hbm.at[k * size : (k + 1) * size, :],
            rows_ref.at[k * size : (k + 1) * size, :],
            row_sems.at[k],
        )
        for k in range(LOADS)
    ]
    sources = (gate_hbm, got_gate_hbm, up_hbm, got_up_hbm)
    copies = [
        pltpu.make_async_copy(ref.at[core], weight_ref.at[k * FF_DEV : (k + 1) * FF_DEV, :], sems.at[k])
        for k, ref in enumerate(sources)
    ]
    for copy in pieces + copies:
        copy.start()
    i, j = iota((LANES, LANES), 0), iota((LANES, LANES), 1)
    sort = (j == (i & (GROUP - 1)) * QUARTERS + (i >> 5)).astype(F32).astype(BF16)
    for g in range(NGROUPS):
        if g * LANES % size == 0:
            pieces[g * LANES // size].wait()
        block = nn(sort, rows_ref[g * LANES : (g + 1) * LANES, :]).astype(BF16)
        for q in range(QUARTERS):
            x_ref[g * GROUP : (g + 1) * GROUP, q * QW : (q + 1) * QW] = block[
                q * GROUP : (q + 1) * GROUP, :
            ]
    for copy in copies:
        copy.wait()
    both = nt(x_ref[...], weight_ref[...])
    gate, upper = both[:, : 2 * FF_DEV], both[:, 2 * FF_DEV :]
    hidden = (gate / (1.0 + jnp.exp(-gate)) * upper).astype(BF16)
    for d in range(NY):
        out_ref[d] = hidden


def weigh_kernel(routes_ref, scores_ref, chi_ref, clo_ref):
    routes, scores = routes_ref[...], scores_ref[...]
    weights = scores / jnp.sum(scores, 0, keepdims=True) * 2.5
    weight = jnp.zeros((EXPERTS, TOK), F32)
    for k in range(TOPK):
        weight += jnp.where(
            routes[k : k + 1, :] == iota((EXPERTS, TOK), 0), weights[k : k + 1, :], 0.0
        )
    high = weight.astype(BF16)
    rest = weight - high.astype(F32)
    rank = membership(routes, 0)
    half = NC * GROUP
    code = spread_tokens(rank).T[:half].astype(BF16)
    high = spread_tokens(high).T[:half].astype(BF16)
    rest = spread_tokens(rest).T[:half].astype(BF16)
    shape = (EXPERTS, BACK_ROWS)
    owner = ((iota(shape, 1) >> 4) == iota(shape, 0)).astype(F32).astype(BF16)
    found = nn(code, owner)
    token, row = iota((half, BACK_ROWS), 0), iota((half, BACK_ROWS), 1)
    table = (found == (((row >> 1) & 7) + 1).astype(F32)) & ((row & 1) == (token >> 5))
    chi_ref[...] = jnp.where(table, nn(high, owner), 0.0).astype(BF16)
    clo_ref[...] = jnp.where(table, nn(rest, owner), 0.0).astype(BF16)


def down_kernel(hidden_ref, keep_ref, got_ref, out_ref, h_ref, stack_ref):
    for d in range(NY):
        h_ref[:, d * FF_DEV : (d + 1) * FF_DEV] = hidden_ref[d, :, :FF_DEV]
        h_ref[:, (NY + d) * FF_DEV : (NY + d + 1) * FF_DEV] = hidden_ref[d, :, FF_DEV:]
    wide = NY * FF_DEV
    done = (nn(h_ref[:, :wide], keep_ref[...]) + nn(h_ref[:, wide:], got_ref[...])).astype(BF16)
    slots = BATCH * CAP
    for p in range(PARTS):
        for q in range(QUARTERS):
            stack_ref[(p * QUARTERS + q) * slots : (p * QUARTERS + q + 1) * slots, :] = done[
                p * slots : (p + 1) * slots, q * LANES : (q + 1) * LANES
            ]
    shape = (BATCH * NC * BACK, QUARTERS * slots)
    i, j = iota(shape, 0), iota(shape, 1)
    slot = (i >> 1) & 7
    quarter = ((i >> 4) & 1) * 2 + (i & 1)
    place = (j == quarter * slots + (i >> 5) * CAP + slot) & (slot < CAP)
    place = place.astype(F32).astype(BF16)
    for p in range(PARTS):
        out_ref[p * shape[0] : (p + 1) * shape[0], :] = nn(
            place, stack_ref[p * shape[1] : (p + 1) * shape[1], :]
        ).astype(BF16)


def combine_kernel(rows_ref, chi_ref, clo_ref, mine_ref, got_ref, out_ref):
    total = nn(chi_ref[...], rows_ref[...]) + nn(clo_ref[...], rows_ref[...])
    for q in range(NC):
        cols = slice(q * LANES, (q + 1) * LANES)
        out_ref[:, cols] = (
            total[q * GROUP : q * GROUP + TOK, :] + (mine_ref[:, cols] + got_ref[:, cols])
        ).astype(BF16)


def call(kernel, outs, scratch, flops, *args, specs=None, out_specs=None, grant=24):
    return pl.pallas_call(
        kernel,
        out_shape=outs,
        in_specs=specs or [VM] * len(args),
        out_specs=out_specs or jax.tree.map(lambda _: VM, outs),
        scratch_shapes=scratch,
        compiler_params=pltpu.CompilerParams(vmem_limit_bytes=grant << 20),
        cost_estimate=pl.CostEstimate(flops=flops, bytes_accessed=1 << 20, transcendentals=0),
    )(*args)


def out(shape, dtype=BF16):
    return jax.ShapeDtypeStruct(shape, dtype)


def hop(x, axis, size, step):
    return lax.ppermute(x, axis, [(i, (i + step) % size) for i in range(size)])


def body(
    tokens,
    norm_gain,
    routes,
    route_scores,
    expert_gate,
    expert_up,
    expert_down,
    shared_gate,
    shared_up,
    shared_down,
):
    send, normed = call(
        pack_kernel,
        (out((ROWS, QW)), out((TOK, D))),
        [
            pltpu.VMEM((LANES, QW), BF16),
            pltpu.VMEM((TOK, D), BF16),
            pltpu.VMEM((1, D), F32),
            pltpu.VMEM((TOPK, TOK), jnp.int32),
            pltpu.VMEM((ROWS, QW), BF16),
            pltpu.VMEM((TOK, D), BF16),
            pltpu.SemaphoreType.DMA((3,)),
            pltpu.SemaphoreType.DMA((SENDS + 1,)),
        ],
        1 << 30,
        tokens,
        norm_gain.reshape(1, D),
        routes.T,
        specs=[HB] * 3,
        out_specs=(HB, HB),
        grant=62,
    )
    rows = lax.all_to_all(
        send.reshape(EP, PIECE, QW), ("z", "x"), split_axis=0, concat_axis=0, tiled=True
    ).reshape(ROWS, QW)
    messages = list(
        call(
            side_kernel,
            tuple(out((MSG, OUT_W)) for _ in range(NY)),
            [pltpu.VMEM((TOK, D), BF16)],
            1 << 30,
            normed,
            shared_gate,
            shared_up,
            shared_down,
            expert_down,
        )
    )
    for d in ORDER[1:]:
        messages[d] = hop(messages[d], "y", NY, d)
    got_gate = hop(expert_gate, "c", NC, 1)
    got_up = hop(expert_up, "c", NC, 1)
    chi, clo = call(
        weigh_kernel,
        (out((NC * GROUP, BACK_ROWS)), out((NC * GROUP, BACK_ROWS))),
        [],
        1 << 28,
        routes.T,
        route_scores.T,
    )
    wide = NY * FF_DEV
    keep, give, mine, other = call(
        ready_kernel,
        (
            out((wide, OUT_W)),
            out((wide, OUT_W)),
            out((TOK, HALF), F32),
            out((TOK, HALF), F32),
        ),
        [],
        1 << 28,
        *[messages[d] for d in ORDER],
    )
    got, other = hop(give, "c", NC, 1), hop(other, "c", NC, 1)
    hidden = call(
        hidden_kernel,
        out((NY, SLOTS, 2 * FF_DEV)),
        [
            pltpu.VMEM((ROWS, QW), BF16),
            pltpu.VMEM((SLOTS, D), BF16),
            pltpu.VMEM((4 * FF_DEV, D), BF16),
            pltpu.SemaphoreType.DMA((LOADS,)),
            pltpu.SemaphoreType.DMA((4,)),
        ],
        1 << 30,
        rows,
        expert_gate,
        got_gate,
        expert_up,
        got_up,
        keep,
        specs=[HB] * 6,
        grant=51,
    )
    hidden = lax.all_to_all(hidden, "y", split_axis=0, concat_axis=0, tiled=True)
    back = call(
        down_kernel,
        out((BACK_ROWS, LANES)),
        [pltpu.VMEM((SLOTS, 2 * wide), BF16), pltpu.VMEM((QUARTERS * SLOTS, LANES), BF16)],
        1 << 30,
        hidden,
        keep,
        got,
    )
    back = lax.all_to_all(
        back.reshape(EXPERTS, BACK, LANES), ("z", "x", "c"), split_axis=0, concat_axis=0, tiled=True
    ).reshape(BACK_ROWS, LANES)
    return call(combine_kernel, out((TOK, HALF)), [], 1 << 28, back, chi, clo, mine, other)


def solution(mesh):
    fine = Mesh(mesh.devices.reshape(NZ, NX, NY, NC), ("z", "x", "y", "c"))
    ep, tp = ("z", "x"), ("y", "c")
    in_specs = (
        P(ep, None),
        P(),
        P(ep, None),
        P(ep, None),
        P(ep, tp, None),
        P(ep, tp, None),
        P(ep, tp, None),
        P(tp, None),
        P(tp, None),
        P(tp, None),
    )
    return jax.shard_map(body, mesh=fine, in_specs=in_specs, out_specs=P(ep, tp), check_vma=False)
```

```python
import jax
import jax.numpy as jnp
from jax import lax
from jax.experimental import pallas as pl
from jax.experimental.pallas import tpu as pltpu
from jax.sharding import Mesh, PartitionSpec as P


NZ, NX, NY, NC = 8, 4, 8, 2
EP = NZ * NX
D = 4096
FF_DEV = 64
TOK = 24
TOPK = 6
EXPERTS = 64
CAP = 6
QUARTERS = 4
QW = D // QUARTERS
PIECE = CAP * QUARTERS
ROWS = EP * PIECE
SLOTS = EP * CAP
OUT_W = D // NY
HALF = OUT_W // NC
LANES = 128
GROUP = 32
NGROUPS = SLOTS // GROUP
MSG = NC * FF_DEV + TOK
ORDER = (0, 4, 5, 3, 6, 2, 7, 1)
SENDS = 4
LOADS = 3
BATCH = 8
PARTS = EP // BATCH
BACK = 16
BACK_ROWS = EXPERTS * BACK
VM = pl.BlockSpec(memory_space=pltpu.VMEM)
HB = pl.BlockSpec(memory_space=pltpu.HBM)
F32, BF16 = jnp.float32, jnp.bfloat16


def iota(shape, dim):
    return lax.broadcasted_iota(jnp.int32, shape, dim)


def nt(a, b):
    return lax.dot_general(a, b, (((1,), (1,)), ((), ())), preferred_element_type=F32)


def nn(a, b):
    return jnp.dot(a, b, preferred_element_type=F32)


def place_of(expert):
    owner = expert >> 1
    return (owner & (NX - 1)) * NZ + (owner >> 2)


def spread_tokens(values):
    lane, token = iota((TOK, LANES), 1), iota((TOK, LANES), 0)
    place = ((lane & (GROUP - 1)) == token).astype(F32).astype(BF16)
    return nn(values.astype(BF16), place)


def membership(routes, base):
    named = jnp.zeros((EXPERTS, TOK), F32)
    for k in range(TOPK):
        named += (routes[k : k + 1, :] == iota((EXPERTS, TOK), 0)).astype(F32)
    earlier = (iota((TOK, TOK), 0) < iota((TOK, TOK), 1)).astype(F32)
    rank = nn(named.astype(BF16), earlier.astype(BF16))
    return named * (rank + 1.0 + (base * place_of(iota((EXPERTS, TOK), 0))).astype(F32))


def pack_kernel(
    tok_hbm,
    gain_hbm,
    routes_hbm,
    send_hbm,
    normed_hbm,
    stack_ref,
    tok_ref,
    gain_ref,
    routes_ref,
    send_ref,
    normed_ref,
    sems,
    out_sems,
):
    core = lax.axis_index("c")
    routes_copy = pltpu.make_async_copy(routes_hbm, routes_ref, sems.at[2])
    tok_copy = pltpu.make_async_copy(tok_hbm, tok_ref, sems.at[0])
    gain_copy = pltpu.make_async_copy(gain_hbm, gain_ref, sems.at[1])
    routes_copy.start()
    tok_copy.start()
    gain_copy.start()
    stack_ref[...] = jnp.zeros(stack_ref.shape, BF16)
    row, expert = iota((ROWS, EXPERTS), 0), iota((ROWS, EXPERTS), 1)
    low = place_of(expert) * PIECE
    owner = ((expert & 1) == core) & (row >= low) & (row < low + PIECE)
    owner = owner.astype(F32).astype(BF16)
    routes_copy.wait()
    code = spread_tokens(membership(routes_ref[...], CAP)).astype(BF16)
    found = nn(owner, code)
    row, col = iota((ROWS, LANES), 0), iota((ROWS, LANES), 1)
    table = (found == ((row >> 2) + 1).astype(F32)) & ((row & 3) == (col >> 5))
    table = table.astype(F32).astype(BF16)
    tok_copy.wait()
    gain_copy.wait()
    values = tok_ref[...].astype(F32)
    normed = (
        values * lax.rsqrt(jnp.mean(values * values, -1, keepdims=True) + 1e-06) * gain_ref[...]
    ).astype(BF16)
    normed_ref[...] = normed
    for q in range(QUARTERS):
        stack_ref[q * GROUP : q * GROUP + TOK, :] = normed[:, q * QW : (q + 1) * QW]
    chunk = ROWS // SENDS
    copies = []
    for k in range(SENDS):
        rows = slice(k * chunk, (k + 1) * chunk)
        send_ref[rows, :] = nn(table[rows, :], stack_ref[...]).astype(BF16)
        copies.append(
            pltpu.make_async_copy(send_ref.at[rows, :], send_hbm.at[rows, :], out_sems.at[k])
        )
        copies[k].start()
    copies.append(pltpu.make_async_copy(normed_ref, normed_hbm, out_sems.at[SENDS]))
    copies[SENDS].start()
    for copy in copies:
        copy.wait()


def side_kernel(normed_ref, sg_ref, su_ref, sd_ref, down_ref, *refs):
    messages, part_ref = refs[:NY], refs[NY]
    me = lax.axis_index("y")
    normed = normed_ref[...]
    gate, upper = nt(normed, sg_ref[...]), nt(normed, su_ref[...])
    hidden = (gate / (1.0 + jnp.exp(-gate)) * upper).astype(BF16)
    part_ref[...] = nn(hidden, sd_ref[...]).astype(BF16)
    for d in range(NY):
        cols = pl.ds(pl.multiple_of(lax.rem(me + d, NY) * OUT_W, OUT_W), OUT_W)
        messages[d][0:FF_DEV, :] = down_ref[0, :, cols]
        messages[d][FF_DEV : 2 * FF_DEV, :] = down_ref[1, :, cols]
        messages[d][2 * FF_DEV : MSG, :] = part_ref[:, cols]


def ready_kernel(*refs):
    messages = dict(zip(ORDER, refs))
    keep_ref, give_ref, mine_ref, other_ref = refs[NY:]
    core, me = lax.axis_index("c"), lax.axis_index("y")
    shared = jnp.zeros((TOK, OUT_W), F32)
    for d in range(NY):
        source = lax.rem(me + NY - d, NY)
        rows = pl.ds(pl.multiple_of(source * FF_DEV, FF_DEV), FF_DEV)
        keep_ref[rows, :] = messages[d][pl.ds(pl.multiple_of(core * FF_DEV, FF_DEV), FF_DEV), :]
        give_ref[rows, :] = messages[d][
            pl.ds(pl.multiple_of((1 - core) * FF_DEV, FF_DEV), FF_DEV), :
        ]
        shared += messages[d][2 * FF_DEV : MSG, :].astype(F32)
    for half in range(NC):

        @pl.when(core == half)
        def _():
            mine_ref[...] = shared[:, half * HALF : (half + 1) * HALF]

        @pl.when(core != half)
        def _():
            other_ref[...] = shared[:, half * HALF : (half + 1) * HALF]


def hidden_kernel(
    rows_hbm, gate_hbm, got_gate_hbm, up_hbm, got_up_hbm, after_hbm, out_ref, rows_ref, x_ref, weight_ref, row_sems, sems
):
    core = lax.axis_index("c")
    size = ROWS // LOADS
    pieces = [
        pltpu.make_async_copy(
            rows_hbm.at[k * size : (k + 1) * size, :],
            rows_ref.at[k * size : (k + 1) * size, :],
            row_sems.at[k],
        )
        for k in range(LOADS)
    ]
    sources = (gate_hbm, got_gate_hbm, up_hbm, got_up_hbm)
    copies = [
        pltpu.make_async_copy(ref.at[core], weight_ref.at[k * FF_DEV : (k + 1) * FF_DEV, :], sems.at[k])
        for k, ref in enumerate(sources)
    ]
    for copy in pieces + copies:
        copy.start()
    i, j = iota((LANES, LANES), 0), iota((LANES, LANES), 1)
    sort = (j == (i & (GROUP - 1)) * QUARTERS + (i >> 5)).astype(F32).astype(BF16)
    for g in range(NGROUPS):
        if g * LANES % size == 0:
            pieces[g * LANES // size].wait()
        block = nn(sort, rows_ref[g * LANES : (g + 1) * LANES, :]).astype(BF16)
        for q in range(QUARTERS):
            x_ref[g * GROUP : (g + 1) * GROUP, q * QW : (q + 1) * QW] = block[
                q * GROUP : (q + 1) * GROUP, :
            ]
    for copy in copies:
        copy.wait()
    both = nt(x_ref[...], weight_ref[...])
    gate, upper = both[:, : 2 * FF_DEV], both[:, 2 * FF_DEV :]
    hidden = (gate / (1.0 + jnp.exp(-gate)) * upper).astype(BF16)
    for d in range(NY):
        out_ref[d] = hidden


def weigh_kernel(routes_ref, scores_ref, chi_ref, clo_ref):
    routes, scores = routes_ref[...], scores_ref[...]
    weights = scores / jnp.sum(scores, 0, keepdims=True) * 2.5
    weight = jnp.zeros((EXPERTS, TOK), F32)
    for k in range(TOPK):
        weight += jnp.where(
            routes[k : k + 1, :] == iota((EXPERTS, TOK), 0), weights[k : k + 1, :], 0.0
        )
    high = weight.astype(BF16)
    rest = weight - high.astype(F32)
    rank = membership(routes, 0)
    half = NC * GROUP
    code = spread_tokens(rank).T[:half].astype(BF16)
    high = spread_tokens(high).T[:half].astype(BF16)
    rest = spread_tokens(rest).T[:half].astype(BF16)
    shape = (EXPERTS, BACK_ROWS)
    expert = iota(shape, 0)
    owner = (iota(shape, 1) >> 4) == place_of(expert) * NC + (expert & 1)
    owner = owner.astype(F32).astype(BF16)
    found = nn(code, owner)
    token, row = iota((half, BACK_ROWS), 0), iota((half, BACK_ROWS), 1)
    table = (found == (((row >> 1) & 7) + 1).astype(F32)) & ((row & 1) == (token >> 5))
    chi_ref[...] = jnp.where(table, nn(high, owner), 0.0).astype(BF16)
    clo_ref[...] = jnp.where(table, nn(rest, owner), 0.0).astype(BF16)


def down_kernel(hidden_ref, keep_ref, got_ref, out_ref, h_ref, stack_ref):
    for d in range(NY):
        h_ref[:, d * FF_DEV : (d + 1) * FF_DEV] = hidden_ref[d, :, :FF_DEV]
        h_ref[:, (NY + d) * FF_DEV : (NY + d + 1) * FF_DEV] = hidden_ref[d, :, FF_DEV:]
    wide = NY * FF_DEV
    done = (nn(h_ref[:, :wide], keep_ref[...]) + nn(h_ref[:, wide:], got_ref[...])).astype(BF16)
    slots = BATCH * CAP
    for p in range(PARTS):
        for q in range(QUARTERS):
            stack_ref[(p * QUARTERS + q) * slots : (p * QUARTERS + q + 1) * slots, :] = done[
                p * slots : (p + 1) * slots, q * LANES : (q + 1) * LANES
            ]
    shape = (BATCH * NC * BACK, QUARTERS * slots)
    i, j = iota(shape, 0), iota(shape, 1)
    slot = (i >> 1) & 7
    quarter = ((i >> 4) & 1) * 2 + (i & 1)
    place = (j == quarter * slots + (i >> 5) * CAP + slot) & (slot < CAP)
    place = place.astype(F32).astype(BF16)
    for p in range(PARTS):
        out_ref[p * shape[0] : (p + 1) * shape[0], :] = nn(
            place, stack_ref[p * shape[1] : (p + 1) * shape[1], :]
        ).astype(BF16)


def combine_kernel(rows_ref, chi_ref, clo_ref, mine_ref, got_ref, out_ref):
    total = nn(chi_ref[...], rows_ref[...]) + nn(clo_ref[...], rows_ref[...])
    for q in range(NC):
        cols = slice(q * LANES, (q + 1) * LANES)
        out_ref[:, cols] = (
            total[q * GROUP : q * GROUP + TOK, :] + (mine_ref[:, cols] + got_ref[:, cols])
        ).astype(BF16)


def call(kernel, outs, scratch, flops, *args, specs=None, out_specs=None, grant=24):
    return pl.pallas_call(
        kernel,
        out_shape=outs,
        in_specs=specs or [VM] * len(args),
        out_specs=out_specs or jax.tree.map(lambda _: VM, outs),
        scratch_shapes=scratch,
        compiler_params=pltpu.CompilerParams(vmem_limit_bytes=grant << 20),
        cost_estimate=pl.CostEstimate(flops=flops, bytes_accessed=1 << 20, transcendentals=0),
    )(*args)


def out(shape, dtype=BF16):
    return jax.ShapeDtypeStruct(shape, dtype)


def hop(x, axis, size, step):
    return lax.ppermute(x, axis, [(i, (i + step) % size) for i in range(size)])


def body(
    tokens,
    norm_gain,
    routes,
    route_scores,
    expert_gate,
    expert_up,
    expert_down,
    shared_gate,
    shared_up,
    shared_down,
):
    send, normed = call(
        pack_kernel,
        (out((ROWS, QW)), out((TOK, D))),
        [
            pltpu.VMEM((LANES, QW), BF16),
            pltpu.VMEM((TOK, D), BF16),
            pltpu.VMEM((1, D), F32),
            pltpu.VMEM((TOPK, TOK), jnp.int32),
            pltpu.VMEM((ROWS, QW), BF16),
            pltpu.VMEM((TOK, D), BF16),
            pltpu.SemaphoreType.DMA((3,)),
            pltpu.SemaphoreType.DMA((SENDS + 1,)),
        ],
        1 << 30,
        tokens,
        norm_gain.reshape(1, D),
        routes.T,
        specs=[HB] * 3,
        out_specs=(HB, HB),
        grant=62,
    )
    rows = lax.all_to_all(
        send.reshape(EP, PIECE, QW), ("x", "z"), split_axis=0, concat_axis=0, tiled=True
    ).reshape(ROWS, QW)
    messages = list(
        call(
            side_kernel,
            tuple(out((MSG, OUT_W)) for _ in range(NY)),
            [pltpu.VMEM((TOK, D), BF16)],
            1 << 30,
            normed,
            shared_gate,
            shared_up,
            shared_down,
            expert_down,
        )
    )
    for d in ORDER[1:]:
        messages[d] = hop(messages[d], "y", NY, d)
    got_gate = hop(expert_gate, "c", NC, 1)
    got_up = hop(expert_up, "c", NC, 1)
    chi, clo = call(
        weigh_kernel,
        (out((NC * GROUP, BACK_ROWS)), out((NC * GROUP, BACK_ROWS))),
        [],
        1 << 28,
        routes.T,
        route_scores.T,
    )
    wide = NY * FF_DEV
    keep, give, mine, other = call(
        ready_kernel,
        (
            out((wide, OUT_W)),
            out((wide, OUT_W)),
            out((TOK, HALF), F32),
            out((TOK, HALF), F32),
        ),
        [],
        1 << 28,
        *[messages[d] for d in ORDER],
    )
    got, other = hop(give, "c", NC, 1), hop(other, "c", NC, 1)
    hidden = call(
        hidden_kernel,
        out((NY, SLOTS, 2 * FF_DEV)),
        [
            pltpu.VMEM((ROWS, QW), BF16),
            pltpu.VMEM((SLOTS, D), BF16),
            pltpu.VMEM((4 * FF_DEV, D), BF16),
            pltpu.SemaphoreType.DMA((LOADS,)),
            pltpu.SemaphoreType.DMA((4,)),
        ],
        1 << 30,
        rows,
        expert_gate,
        got_gate,
        expert_up,
        got_up,
        keep,
        specs=[HB] * 6,
        grant=51,
    )
    hidden = lax.all_to_all(hidden, "y", split_axis=0, concat_axis=0, tiled=True)
    back = call(
        down_kernel,
        out((BACK_ROWS, LANES)),
        [pltpu.VMEM((SLOTS, 2 * wide), BF16), pltpu.VMEM((QUARTERS * SLOTS, LANES), BF16)],
        1 << 30,
        hidden,
        keep,
        got,
    )
    back = lax.all_to_all(
        back.reshape(EXPERTS, BACK, LANES), ("x", "z", "c"), split_axis=0, concat_axis=0, tiled=True
    ).reshape(BACK_ROWS, LANES)
    return call(combine_kernel, out((TOK, HALF)), [], 1 << 28, back, chi, clo, mine, other)


def solution(mesh):
    fine = Mesh(mesh.devices.reshape(NZ, NX, NY, NC), ("z", "x", "y", "c"))
    ep, tp = ("z", "x"), ("y", "c")
    in_specs = (
        P(ep, None),
        P(),
        P(ep, None),
        P(ep, None),
        P(ep, tp, None),
        P(ep, tp, None),
        P(ep, tp, None),
        P(tp, None),
        P(tp, None),
        P(tp, None),
    )
    return jax.shard_map(body, mesh=fine, in_specs=in_specs, out_specs=P(ep, tp), check_vma=False)
```
